32 devices in a mesh: sp: 8 (over z, x), tp: 4 (over y, core).
Axes of the slice: x: 2, y: 2, z: 4, core: 2. Of those that a mesh axis runs over, the one named last changes fastest.
Arguments:
- in_gate: bfloat16 [1024, 2048], P('tp', 'sp'), may hold values from -6 to 6
- out_gate: bfloat16 [1024, 2048], P('tp', 'sp'), may hold values from -6 to 6
- values: bfloat16 [1024, 2048], P('tp', 'sp'), may hold values from -6 to 6
- conv_taps: bfloat16 [3, 1024], P(None, 'tp'), may hold values from -3.5 to 3.5
- doc_ids: int32 [2048], P('sp'), may hold values from 0 to 1, as said below
- residual: bfloat16 [2048, 2048], P('sp'), may hold values from -6 to 6
- out_weight: bfloat16 [1024, 2048], P('tp'), may hold values from -0.1875 to 0.1875
- norm_gain: bfloat16 [2048], replicated, may hold values from 0.099609375 to 1.8984375
- routes: int32 [2048, 2], P('sp'), may hold values from 0 to 7, all different within a row; in each aligned block of 256 rows (0 to 255, 256 to 511, ...) at most 96 rows name the same one
- route_weights: float32 [2048, 2], P('sp'), may hold values from 0.2 to 1
- expert_gate: bfloat16 [8, 2048, 4224], P('sp', None, 'tp'), may hold values from -0.125 to 0.125
- expert_up: bfloat16 [8, 2048, 4224], P('sp', None, 'tp'), may hold values from -0.125 to 0.125
- expert_down: bfloat16 [8, 4224, 2048], P('sp', 'tp'), may hold values from -0.09375 to 0.09375
Outputs:
- merged: bfloat16 [2048, 2048], P('sp', 'tp')
The draws below stay inside these ranges and needn't reach their ends.
Inputs may be any that keep to these rules, and one draw needn't show every extreme that they name: `routes`: each row names 2 different experts. Within the rows of one index of sp (aligned blocks of 256 rows) no expert is named more than 96 times, a bound that some expert reaches in some blocks. `doc_ids`: never falls along the sequence; starts at 0 and rises by one at each of 1 document starts, each number used.
All inputs are finite; a program needn't handle non-finite values.
Results may differ from the reference program's by a relative error of at most 0.019.
Values may be sent and summed in bfloat16 or wider, within the bound.
A program may use at most 64 MiB of HBM per device.

```python
import math
import jax
import jax.numpy as jnp
import numpy as np
from jax import lax

D = 2048
D_CONV = 1024
FF = 4224
TOP = 2
TOK_SP = 256
TOKENS = 2048
EXPERTS = 8
CAP = 96
DOCS = 2
N_SP = 8
N_TP = 4


def draw_doc_ids(key, part):
    starts = jax.random.permutation(jax.random.fold_in(key, 17), TOKENS - 1)[:DOCS - 1].astype(jnp.int32) + 1
    positions = jnp.arange(TOKENS, dtype=jnp.int32)
    return jnp.sum((positions[:, None] >= starts[None, :]).astype(jnp.int32), axis=1).astype(jnp.int32)


def shard_levels(key, extent, cuts, low, largest):
    factor_of = 1.0
    for axis_at, blocks in cuts:
        heights = jax.random.uniform(jax.random.fold_in(jax.random.fold_in(key, 6), axis_at), (blocks,), jnp.float32, low / len(cuts), largest / len(cuts))
        factor_of = factor_of * jnp.repeat(jnp.exp(heights), extent[axis_at] // blocks).reshape((-1,) + (1,) * (len(extent) - 1 - axis_at))
    return factor_of


def assign_block(own_key, own, number, rows, number_of, top, reach, slope):
    order = jax.random.permutation(own_key, number_of)
    crowded, usual = shares(number_of, rows * top, reach, slope, True), shares(number_of, rows * top, reach, slope, False)
    places = jnp.arange(number_of)

    def named(sizes, offset_by):
        used = int((sizes > 0).sum())
        fixed = max(1, used // 4)
        moved = fixed + (places - fixed + offset_by * (used - fixed)) % max(1, number_of - fixed)
        return jnp.zeros((number_of,), jnp.int32).at[order[jnp.where(places < fixed, places, moved)]].set(jnp.asarray(sizes, jnp.int32))

    sizes = jnp.where(number % 4 == 0, named(crowded, number // 4), named(usual, number - number // 4 - 1))
    mixed = jax.random.permutation(jax.random.fold_in(own, 3), number_of)
    source_of, sink = mixed[0:number_of // 2 * 2:2], mixed[1:number_of // 2 * 2:2]
    room = jnp.minimum(sizes[source_of] - 1, reach - sizes[sink]) // 2
    room = jnp.where((source_of == order[0]) | (sink == order[0]) | (sizes[sink] == 0), 0, jnp.maximum(room, 0))
    moved = jax.random.randint(jax.random.fold_in(own, 4), (number_of // 2,), 0, 1 << 20) % (room + 1)
    sizes = sizes.at[source_of].add(-moved).at[sink].add(moved)
    labels = jnp.searchsorted(jnp.cumsum(sizes), jnp.arange(rows * top), side="right").astype(jnp.int32)
    grid = labels.reshape(top, rows).T
    grid = grid[jax.random.permutation(jax.random.fold_in(own, 1), rows)]
    offset_by = jax.random.randint(jax.random.fold_in(own, 2), (rows, 1), 0, top)
    return jnp.take_along_axis(grid, (jnp.arange(top)[None, :] + offset_by) % top, axis=1)


def shares(number_of, total, reach, slope, full):
    portions = [(1 << 20) // math.isqrt(grade ** slope) + 1 for grade in range(1, number_of + 1)]
    largest = reach if full else min(reach, max(-(-total // number_of), total * portions[0] // sum(portions)))
    least = 1 if total - largest >= number_of - 1 else 0
    given, rest = [largest] + [least] * (number_of - 1), total - largest - least * (number_of - 1)
    while rest > 0:
        candidates = [i for i in range(1, number_of) if given[i] < largest] or [i for i in range(1, number_of) if given[i] < reach]
        mass, budget = sum([portions[i] for i in candidates]), rest
        for i in candidates:
            more = min(reach - given[i], max(1, budget * portions[i] // mass), rest)
            given[i] = given[i] + more
            rest = rest - more
    return np.array(given)


def centred(key, extent, deviation, most, shards=(), kind=jnp.bfloat16):
    result = deviation * jax.random.normal(key, extent, jnp.float32)
    if shards:
        result = result * shard_levels(key, extent, shards, -0.22, 0.18)
    return jnp.clip(result, -most, most).astype(kind)


def setup_inputs(seed: int = 0) -> dict:
    key_list = jax.random.split(jax.random.key(seed), 14)
    in_gate = centred(key_list[0], (D_CONV, TOKENS), 1.0, 6.0, ((0, 4), (1, 8)))
    out_gate = centred(key_list[1], (D_CONV, TOKENS), 1.0, 6.0, ((0, 4), (1, 8)))
    values = centred(key_list[2], (D_CONV, TOKENS), 1.0, 6.0, ((0, 4), (1, 8)))
    conv_taps = centred(key_list[3], (3, D_CONV), 3 ** -0.5, 3.5, ((1, 4),))
    doc_ids = draw_doc_ids(jax.random.fold_in(key_list[13], 71), 0)
    residual = centred(key_list[5], (TOKENS, D), 1.0, 6.0, ((0, 8),))
    out_weight = centred(key_list[6], (D_CONV, D), D_CONV ** -0.5, 0.1875, ((0, 4),))
    norm_gain = jnp.clip(1.0 + 0.18 * jax.random.normal(key_list[7], (D,), jnp.float32), 0.099609375, 1.8984375).astype(jnp.bfloat16)
    routes_keys = jax.random.split(jax.random.fold_in(key_list[8], 1), TOKENS // TOK_SP)
    routes_turns = jax.random.permutation(jax.random.fold_in(key_list[8], 3), TOKENS // TOK_SP)
    routes = jax.vmap(lambda own, number: assign_block(jax.random.fold_in(key_list[8], 2), own, number, TOK_SP, EXPERTS, TOP, CAP, 1))(routes_keys, routes_turns).reshape((TOKENS, TOP))
    route_weights = jnp.clip(0.2 + 0.8 * jax.random.uniform(key_list[9], (TOKENS, TOP), jnp.float32) ** shard_levels(key_list[9], (TOKENS, TOP), ((0, 8),), -0.2, 0.2), 0.2, 1.0)
    expert_gate = centred(key_list[10], (EXPERTS, D, FF), D ** -0.5, 0.125, ((0, 8), (2, 4)))
    expert_up = centred(key_list[11], (EXPERTS, D, FF), D ** -0.5, 0.125, ((0, 8), (2, 4)))
    expert_down = centred(key_list[12], (EXPERTS, FF, D), FF ** -0.5, 0.09375, ((0, 8), (1, 4)))
    return {"in_gate": in_gate, "out_gate": out_gate, "values": values, "conv_taps": conv_taps, "doc_ids": doc_ids, "residual": residual, "out_weight": out_weight, "norm_gain": norm_gain, "routes": routes, "route_weights": route_weights, "expert_gate": expert_gate, "expert_up": expert_up, "expert_down": expert_down}


EPSILON = 1e-06

def reference(in_gate, out_gate, values, conv_taps, doc_ids, residual, out_weight, norm_gain, routes, route_weights, expert_gate, expert_up, expert_down):
    gated_in = (in_gate.astype(jnp.float32) * values.astype(jnp.float32)).astype(jnp.bfloat16)
    gated_f = lax.optimization_barrier(gated_in).astype(jnp.float32)
    length = doc_ids.shape[0]
    shift_one = jnp.pad(gated_f, ((0, 0), (1, 0)))[:, :length]
    shift_two = jnp.pad(gated_f, ((0, 0), (2, 0)))[:, :length]
    docs_one = jnp.pad(doc_ids, (1, 0), constant_values=-1)[:length]
    docs_two = jnp.pad(doc_ids, (2, 0), constant_values=-1)[:length]
    near_mask = (docs_one == doc_ids).astype(jnp.float32)
    far_mask = (docs_two == doc_ids).astype(jnp.float32)
    tap_values = conv_taps.astype(jnp.float32)
    convolved = tap_values[2][:, None] * gated_f + tap_values[1][:, None] * shift_one * near_mask[None, :] + tap_values[0][:, None] * shift_two * far_mask[None, :]
    mixed_rows = (out_gate.astype(jnp.float32) * convolved).astype(jnp.bfloat16)
    projected = jnp.dot(mixed_rows.T, out_weight, preferred_element_type=jnp.float32)
    stream = residual.astype(jnp.float32) + projected
    inv_rms = lax.rsqrt(lax.optimization_barrier(jnp.mean(stream * stream, axis=1, keepdims=True)) + EPSILON)
    normed = (stream * inv_rms * norm_gain.astype(jnp.float32)[None, :]).astype(jnp.bfloat16)
    total_rows = N_SP * CAP
    hidden_block = FF // N_TP

    def one_expert(expert):
        hit_table = routes == expert
        weight_row = lax.optimization_barrier(jnp.sum(jnp.where(hit_table, route_weights, jnp.float32(0.0)), axis=1))
        used_rows = jnp.any(hit_table, axis=1)
        picked = jnp.nonzero(used_rows, size=total_rows, fill_value=0)[0].astype(jnp.int32)
        live_rows = (jnp.arange(total_rows) < jnp.sum(used_rows.astype(jnp.int32))).astype(jnp.float32)
        row_block = jnp.take(normed, picked, axis=0)
        gate_sum = jnp.dot(row_block, expert_gate[expert], preferred_element_type=jnp.float32)
        up_sum = jnp.dot(row_block, expert_up[expert], preferred_element_type=jnp.float32)
        hidden = (jax.nn.silu(gate_sum) * up_sum).astype(jnp.bfloat16)
        pieces = jnp.einsum('rnf,nfd->nrd', hidden.astype(jnp.float32).reshape(total_rows, N_TP, hidden_block), expert_down[expert].astype(jnp.float32).reshape(N_TP, hidden_block, D))
        pieces = lax.optimization_barrier(pieces.astype(jnp.bfloat16)).astype(jnp.float32)
        summed = lax.optimization_barrier(lax.optimization_barrier(jnp.sum(pieces, axis=0)).astype(jnp.bfloat16)).astype(jnp.float32)
        return (picked, (jnp.take(weight_row, picked) * live_rows)[:, None] * summed)
    picked_all, terms = lax.map(one_expert, jnp.arange(EXPERTS, dtype=jnp.int32))
    blended = jnp.zeros_like(stream).at[picked_all.reshape(-1)].add(terms.reshape(-1, D))
    return (stream + blended).astype(jnp.bfloat16)
```

```python
import functools

import jax
import jax.numpy as jnp
from jax import lax
from jax.experimental import pallas as pl
from jax.experimental.pallas import tpu as pltpu
from jax.sharding import PartitionSpec as P

EPSILON = 1e-06


def shifted(x, axis, by):
    count = lax.axis_size(axis)
    pairs = [(i, i + by) for i in range(count) if 0 <= i + by < count]
    return lax.ppermute(x, axis, pairs)


def shards(
    in_gate,
    out_gate,
    values,
    conv_taps,
    doc_ids,
    residual,
    out_weight,
    norm_gain,
    routes,
    route_weights,
    expert_gate,
    expert_up,
    expert_down,
):
    gated_in = (in_gate.astype(jnp.float32) * values.astype(jnp.float32)).astype(jnp.bfloat16)
    tail_rows, tail_docs = shifted((gated_in[:, -2:], doc_ids[-2:]), "sp", 1)
    extended = lax.optimization_barrier(jnp.concatenate([tail_rows, gated_in], axis=1)).astype(
        jnp.float32
    )
    docs_ext = jnp.concatenate([tail_docs, doc_ids])
    length = doc_ids.shape[0]
    near_mask = (docs_ext[1 : length + 1] == doc_ids).astype(jnp.float32)
    far_mask = (docs_ext[0:length] == doc_ids).astype(jnp.float32)
    tap_values = conv_taps.astype(jnp.float32)
    convolved = (
        tap_values[2][:, None] * extended[:, 2:]
        + tap_values[1][:, None] * extended[:, 1 : length + 1] * near_mask[None, :]
        + tap_values[0][:, None] * extended[:, 0:length] * far_mask[None, :]
    )
    mixed_rows = (out_gate.astype(jnp.float32) * convolved).astype(jnp.bfloat16)
    partial_value = lax.dot_general(
        mixed_rows, out_weight, (((0,), (0,)), ((), ())), preferred_element_type=jnp.float32
    )
    tp_count = lax.axis_size("tp")
    model_width = residual.shape[1]
    share_width = model_width // tp_count
    column = lax.axis_index("tp") * share_width
    stream = residual.astype(jnp.float32) + lax.psum(
        partial_value.astype(jnp.bfloat16), "tp"
    ).astype(jnp.float32)
    inv_rms = lax.rsqrt(jnp.mean(stream * stream, axis=1, keepdims=True) + EPSILON)
    normed = (stream * inv_rms * norm_gain.astype(jnp.float32)[None, :]).astype(jnp.bfloat16)
    stream_cols = lax.dynamic_slice_in_dim(stream, column, share_width, 1)
    own_cols = lax.dynamic_slice_in_dim(normed, column, share_width, 1)
    tokens = routes.shape[0]
    top_count = routes.shape[1]
    experts = lax.axis_size("sp")
    capacity = 3 * tokens * top_count // (2 * experts)
    chosen = routes.reshape(-1)
    hits_table = (chosen[:, None] == jnp.arange(experts, dtype=jnp.int32)[None, :]).astype(
        jnp.int32
    )
    earlier = jnp.cumsum(hits_table, axis=0) - hits_table
    ranked = jnp.sum(earlier * hits_table, axis=1)
    slot_index = chosen * capacity + ranked
    owners = jnp.arange(tokens * top_count, dtype=jnp.int32) // top_count
    source = jnp.zeros((experts * capacity,), jnp.int32).at[slot_index].set(owners)
    filled = jnp.zeros((experts * capacity,), jnp.bool_).at[slot_index].set(True)
    gate_weight = expert_gate[0]
    up_weight = expert_up[0]
    down_weight = expert_down[0]
    picked = jnp.where(
        filled[:, None], jnp.take(own_cols, source, axis=0), jnp.zeros((), jnp.bfloat16)
    ).reshape(experts, capacity, share_width)
    arrived = lax.all_to_all(picked, "sp", split_axis=0, concat_axis=0, tiled=True)
    slot_count = arrived.shape[1]
    row_block = arrived.reshape(-1, share_width)
    piece_cols = lax.all_gather(row_block, "tp", axis=1, tiled=True)
    gate_sum = jnp.dot(piece_cols, gate_weight, preferred_element_type=jnp.float32)
    up_sum = jnp.dot(piece_cols, up_weight, preferred_element_type=jnp.float32)
    hidden = (jax.nn.silu(gate_sum) * up_sum).astype(jnp.bfloat16)
    down_sum = jnp.dot(hidden, down_weight, preferred_element_type=jnp.float32)
    summed = lax.psum_scatter(down_sum.astype(jnp.bfloat16), "tp", scatter_dimension=1, tiled=True)
    returned = lax.all_to_all(
        summed.reshape(experts, slot_count, share_width),
        "sp",
        split_axis=0,
        concat_axis=0,
        tiled=True,
    )
    results = jnp.take(returned.reshape(experts * capacity, share_width), slot_index, axis=0)
    results = results.astype(jnp.float32).reshape(tokens, top_count, share_width)
    blended = jnp.sum(route_weights[:, :, None] * results, axis=1)
    return (stream_cols + blended).astype(jnp.bfloat16)

MESH = pl.DeviceIdType.MESH
F32 = jnp.float32
BF16 = jnp.bfloat16
LANES = 128


def xor_index(value, mask):
    bit = 1
    while bit <= mask:
        if mask & bit:
            value = value + bit - 2 * bit * lax.rem(lax.div(value, bit), 2)
        bit *= 2
    return value


def column_of(row, width):
    return jnp.transpose(jnp.broadcast_to(row, (LANES, row.shape[1])))[:, :width]


def across_rows(left, right):
    return lax.dot_general(left, right, (((1,), (1,)), ((), ())), preferred_element_type=F32)


def plan_stages(planes):
    far = [(mask, flip) for mask in range(planes // 2, planes) for flip in (0, 1)]
    near = [(0, 1)] + [(mask, flip) for mask in range(1, planes // 2) for flip in (0, 1)] + [(0, 0)]
    return list(zip(far, near))


def layer_kernel(
    sp_count,
    capacity,
    in_gate_ref,
    out_gate_ref,
    values_ref,
    taps_ref,
    docs_ref,
    residual_ref,
    out_weight_ref,
    gain_ref,
    routes_ref,
    weights_ref,
    gate_hbm,
    up_hbm,
    down_hbm,
    out_ref,
    gate_ref,
    up_ref,
    down_ref,
    gains,
    own_residual,
    gated,
    tail,
    halo,
    halo_docs,
    share,
    share_in,
    pair_sum,
    pair_in,
    edge,
    edge_in,
    squares,
    squares_in,
    keys,
    select,
    weight_cols,
    scales,
    scales_in,
    stream,
    picked,
    rows_ref,
    gate_part,
    up_part,
    down_share,
    down_in,
    down_pair,
    down_pair_in,
    finished,
    back,
    halo_send,
    halo_recv,
    local_sem,
    share_send,
    share_recv,
    pair_send,
    pair_recv,
    edge_send,
    edge_recv,
    square_send,
    square_recv,
    scale_send,
    scale_recv,
    row_send,
    row_recv,
    spread_send,
    spread_recv,
    half_send,
    half_recv,
    cross_send,
    cross_recv,
    back_send,
    back_recv,
):
    me = lax.axis_index("sp")
    rank = lax.axis_index("tp")
    side, core = lax.div(rank, 2), lax.rem(rank, 2)
    plane, lane = lax.div(me, 2), lax.rem(me, 2)
    partner = 2 * side + 1 - core
    across = 2 * (1 - side) + core
    diagonal = 2 * (1 - side) + 1 - core
    channels, tokens = in_gate_ref.shape
    model_width = residual_ref.shape[1]
    width = stream.shape[1]
    half_width = width // 2
    places = plan_stages(sp_count // 2)
    stages = len(places)
    own = (stages - 1, 1)

    def cols(owner):
        return pl.ds(pl.multiple_of(owner * width, width), width)

    def chip_cols(which):
        return pl.ds(pl.multiple_of(which * 2 * width, 2 * width), 2 * width)

    def remote(src, dst, send, recv, device):
        return pltpu.make_async_remote_copy(
            src_ref=src, dst_ref=dst, send_sem=send, recv_sem=recv, device_id=device, device_id_type=MESH
        )

    def peer(at):
        mask, flip = places[at[0]][at[1]]
        return 2 * xor_index(plane, mask) + (1 - lane if flip else lane)

    local = [
        pltpu.make_async_copy(residual_ref.at[:, cols(rank)], own_residual, local_sem.at[0]),
        pltpu.make_async_copy(gate_hbm.at[0], gate_ref, local_sem.at[1]),
        pltpu.make_async_copy(up_hbm.at[0], up_ref, local_sem.at[2]),
        pltpu.make_async_copy(down_hbm.at[0], down_ref, local_sem.at[3]),
    ]
    for copy in local:
        copy.start()

    barrier = pltpu.get_barrier_semaphore()
    for step in range(1, sp_count):
        pl.semaphore_signal(
            barrier, inc=1, device_id={"sp": lax.rem(me + step, sp_count)}, device_id_type=MESH
        )
    for other in (partner, across, diagonal):
        pl.semaphore_signal(barrier, inc=1, device_id={"tp": other}, device_id_type=MESH)

    gains[...] = gain_ref[...].astype(F32)
    gated[...] = (in_gate_ref[...].astype(F32) * values_ref[...].astype(F32)).astype(BF16)
    head_rows = tail.shape[0]
    tail[...] = jnp.transpose(gated[:, tokens - LANES :].astype(F32))[LANES - head_rows :, :].astype(
        BF16
    )
    tap_rows = [taps_ref[k : k + 1, :].astype(F32) for k in range(3)]
    wide_taps = [
        jnp.concatenate([column_of(tap, LANES)] * (tokens // LANES), axis=1) for tap in tap_rows
    ]
    docs = jnp.broadcast_to(docs_ref[...], (8, tokens))
    token_row = lax.broadcasted_iota(jnp.int32, (8, tokens), 1)

    def same_document(by):
        alike = (pltpu.roll(docs, by, 1) == docs) & (token_row >= by)
        return jnp.where(alike, 1.0, 0.0)[0:1, :]

    main = gated[...].astype(F32)
    convolved = (
        wide_taps[2] * main
        + wide_taps[1] * pltpu.roll(main, 1, 1) * same_document(1)
        + wide_taps[0] * pltpu.roll(main, 2, 1) * same_document(2)
    )
    mixed = jnp.transpose(out_gate_ref[...].astype(F32) * convolved).astype(BF16)

    def projected(owner):
        return jnp.dot(mixed, out_weight_ref[:, cols(owner)], preferred_element_type=F32)

    halves = [pl.ds(k * half_width, half_width) for k in range(2)]
    to_partner = [
        remote(
            share.at[0, :, halves[k]],
            share_in.at[0, :, halves[k]],
            share_send.at[k],
            share_recv.at[k],
            {"tp": partner},
        )
        for k in range(2)
    ] + [remote(share.at[1], share_in.at[1], share_send.at[2], share_recv.at[2], {"tp": partner})]
    share[0] = projected(diagonal).astype(BF16)
    following = lax.rem(me + 1, sp_count)
    halo_copies = [
        remote(tail, halo, halo_send.at[0], halo_recv.at[0], {"sp": following}),
        remote(docs_ref, halo_docs, halo_send.at[1], halo_recv.at[1], {"sp": following}),
    ]
    pair_copies = [
        remote(
            pair_sum.at[:, halves[k]],
            pair_in.at[:, halves[k]],
            pair_send.at[k],
            pair_recv.at[k],
            {"tp": across},
        )
        for k in range(2)
    ]

    def send_pair(k):
        to_partner[k].wait_recv()
        pair_sum[:, halves[k]] = (
            crossing[:, k * half_width : (k + 1) * half_width]
            + share_in[0, :, halves[k]].astype(F32)
        ).astype(BF16)
        pair_copies[k].start()

    pl.semaphore_wait(barrier, sp_count + 2)
    to_partner[0].start()
    to_partner[1].start()
    for copy in halo_copies:
        copy.start()
    crossing = projected(across)
    send_pair(0)
    share[1] = projected(partner).astype(BF16)
    to_partner[2].start()
    stream[...] = projected(rank)

    for copy in halo_copies:
        copy.wait_recv()
    earlier = jnp.where(me > 0, halo[...].astype(F32), 0.0)
    old_docs = jnp.broadcast_to(halo_docs[...], (8, tokens))[:, tokens - LANES :]
    docs_ext = jnp.concatenate([old_docs, docs[:, :LANES]], axis=1)

    def carried_mask(by):
        alike = pltpu.roll(docs_ext, by, 1)[:, LANES:] == docs[:, :LANES]
        alike = alike & (token_row[:, :LANES] < by)
        return column_of(jnp.where(alike, 1.0, 0.0)[0:1, :], LANES)[0:head_rows, 0:1]

    carried = tap_rows[1] * pltpu.roll(earlier, 1, 0) * carried_mask(1) + tap_rows[0] * pltpu.roll(
        earlier, 2, 0
    ) * carried_mask(2)
    edge_mixed = jnp.transpose(out_gate_ref[:, 0:LANES].astype(F32))[0:head_rows, :] * carried
    edge_mixed = edge_mixed.astype(BF16)

    def edge_projected(owner):
        return jnp.dot(edge_mixed, out_weight_ref[:, cols(owner)], preferred_element_type=F32)

    edge_copies = []
    for k, other in enumerate((across, diagonal, partner)):
        edge[k] = edge_projected(other).astype(BF16)
        copy = remote(edge.at[k], edge_in.at[k], edge_send.at[k], edge_recv.at[k], {"tp": other})
        copy.start()
        edge_copies.append(copy)
    send_pair(1)
    stream[0:head_rows, :] += edge_projected(rank)
    to_partner[2].wait_recv()
    local[0].wait()
    stream[...] += share_in[1].astype(F32) + own_residual[...].astype(F32)

    experts = lax.broadcasted_iota(jnp.int32, (sp_count, tokens), 0)
    hits = jnp.zeros((sp_count, tokens), F32)
    expert_weights = jnp.zeros((sp_count, tokens), F32)
    for k in range(routes_ref.shape[0]):
        named = routes_ref[k : k + 1, :] == experts
        hits = jnp.where(named, 1.0, hits)
        expert_weights = jnp.where(named, weights_ref[k : k + 1, :], expert_weights)
    before = lax.broadcasted_iota(jnp.int32, (tokens, tokens), 0) < lax.broadcasted_iota(
        jnp.int32, (tokens, tokens), 1
    )
    ranks = jnp.dot(
        hits.astype(BF16), jnp.where(before, 1.0, 0.0).astype(BF16), preferred_element_type=F32
    )
    key_rows = jnp.where(hits > 0.5, ranks, -1.0)
    keys[...] = key_rows
    slot_lanes = select.shape[2]
    lanes = lax.broadcasted_iota(jnp.int32, (tokens, slot_lanes), 1)
    slots = jnp.where(lanes < capacity, lanes, lanes - capacity)
    slots = jnp.where(lanes < 2 * capacity, slots, -2).astype(F32)
    for expert_index in range(sp_count):
        one = slice(expert_index, expert_index + 1)
        key_cols = jnp.concatenate(
            [column_of(key_rows[one, :], LANES)] * (slot_lanes // LANES), axis=1
        )
        select[expert_index] = jnp.where(key_cols == slots, 1.0, 0.0).astype(BF16)
        weight_cols[expert_index] = column_of(expert_weights[one, :], LANES)

    per_rank = width // LANES
    gain = jnp.concatenate(
        [gains[pl.ds(rank * per_rank + k, 1), :] for k in range(per_rank)], axis=1
    )
    for copy in edge_copies:
        copy.wait_recv()
    stream[0:head_rows, :] += (
        edge_in[0].astype(F32) + edge_in[1].astype(F32) + edge_in[2].astype(F32)
    )
    for copy in pair_copies:
        copy.wait_recv()
    total = stream[...] + pair_in[...].astype(F32)
    stream[...] = total
    scaled = (total * gain).astype(BF16)

    def place_rows(at):
        return pl.ds(at[1] * capacity, capacity)

    slot_rows = lax.broadcasted_iota(jnp.int32, (capacity, tokens), 0).astype(F32)

    def index(at):
        return 2 * at[0] + at[1]

    def pick(at):
        chosen = jnp.where(keys[pl.ds(peer(at), 1), :] == slot_rows, 1.0, 0.0).astype(BF16)
        return jnp.dot(chosen, scaled, preferred_element_type=F32).astype(BF16)

    def own_block(at):
        return rows_ref.at[at[0], place_rows(at), cols(rank)]

    def row_copy(at):
        return remote(
            picked.at[index(at)],
            own_block(at),
            row_send.at[index(at)],
            row_recv.at[index(at)],
            {"sp": peer(at)},
        )

    def spread(at, kind):
        owner, device = ((rank, across), (rank, partner), (across, partner))[kind]
        block = rows_ref.at[at[0], place_rows(at), cols(owner)]
        p = index(at)
        return remote(
            block, block, spread_send.at[p, kind], spread_recv.at[p, kind], {"tp": device}
        )

    def spread_arrival(at, kind):
        owner = (across, partner, diagonal)[kind]
        block = rows_ref.at[at[0], place_rows(at), cols(owner)]
        p = index(at)
        return remote(
            block, block, spread_send.at[p, kind], spread_recv.at[p, kind], {"tp": partner}
        )

    def send_rows(at):
        if at == own:
            rows_ref[at[0], place_rows(at), cols(rank)] = pick(at)
            spread(at, 0).start()
            spread(at, 1).start()
        else:
            picked[index(at)] = pick(at)
            row_copy(at).start()

    everyone = [(stage, place) for stage in range(stages) for place in range(2)]
    send_order = [(0, 0), (0, 1), own] + [
        at for stage in range(1, stages) for at in ((stage, 1), (stage, 0)) if at != own
    ]
    for at in send_order:
        send_rows(at)

    own_square = jnp.sum(total * total, axis=1, keepdims=True)
    squares[...] = jnp.transpose(jnp.broadcast_to(own_square, (tokens, LANES)))[0:8, :]
    square_copies = [
        remote(
            squares, squares_in.at[k], square_send.at[k], square_recv.at[k], {"tp": other}
        )
        for k, other in enumerate((partner, across, diagonal))
    ]
    for copy in square_copies:
        copy.start()
    for copy in square_copies:
        copy.wait_recv()
    all_squares = squares[...] + squares_in[0] + squares_in[1] + squares_in[2]
    inv_rms = column_of(lax.rsqrt(all_squares / model_width + EPSILON)[0:1, :], LANES)
    inv_cols = jnp.concatenate([inv_rms] * (slot_lanes // LANES), axis=1)

    def scale_copy(at):
        p = index(at)
        return remote(
            scales.at[p], scales_in.at[p], scale_send.at[p], scale_recv.at[p], {"sp": peer(at)}
        )

    for at in send_order:
        row = jnp.sum(select[peer(at)].astype(F32) * inv_cols, axis=0, keepdims=True)
        if at == own:
            scales_in[index(at)] = jnp.broadcast_to(row, scales.shape[1:])
        else:
            scales[index(at)] = jnp.broadcast_to(row, scales.shape[1:])
            scale_copy(at).start()

    def direct(at):
        row_copy(at).wait_recv()
        spread(at, 0).start()
        spread(at, 1).start()

    def relay(at):
        spread_arrival(at, 0).wait_recv()
        spread(at, 2).start()

    def half_copy(stage, k):
        return remote(
            down_share.at[stage, k],
            down_in.at[stage, k],
            half_send.at[stage, k],
            half_recv.at[stage, k],
            {"tp": partner},
        )

    def expert_near(stage):
        for place in range(2):
            spread_arrival((stage, place), 1).wait_recv()
        block = rows_ref[stage, :, chip_cols(side)]
        gate_part[stage % 2] = across_rows(gate_ref[:, chip_cols(side)], block)
        up_part[stage % 2] = across_rows(up_ref[:, chip_cols(side)], block)

    def expert_far(stage):
        for place in range(2):
            spread_arrival((stage, place), 2).wait_recv()
            if (stage, place) != own:
                scale_copy((stage, place)).wait_recv()
        block = rows_ref[stage, :, chip_cols(1 - side)]
        scale_lane = lax.broadcasted_iota(jnp.int32, scales.shape[1:], 1)
        scale = jnp.where(scale_lane < capacity, scales_in[2 * stage], scales_in[2 * stage + 1])
        scale = scale[0:1, 0 : 2 * capacity]
        gate_sum = gate_part[stage % 2] + across_rows(gate_ref[:, chip_cols(1 - side)], block)
        up_sum = up_part[stage % 2] + across_rows(up_ref[:, chip_cols(1 - side)], block)
        gate_sum = gate_sum * scale
        up_sum = up_sum * scale
        hidden = jnp.transpose(gate_sum / (1.0 + jnp.exp(-gate_sum)) * up_sum).astype(BF16)
        for k, owner in enumerate((diagonal, partner, across, rank)):
            down_share[stage, k] = jnp.dot(
                hidden, down_ref[:, cols(owner)], preferred_element_type=F32
            ).astype(BF16)
            if k < 2:
                half_copy(stage, k).start()

    def cross_copy(at):
        return remote(
            down_pair.at[at[0], place_rows(at)],
            down_pair_in.at[at[0], place_rows(at)],
            cross_send.at[index(at)],
            cross_recv.at[index(at)],
            {"tp": across},
        )

    def cross(at):
        stage, rows = at[0], place_rows(at)
        if at[1] == 0:
            half_copy(stage, 0).wait_recv()
        down_pair[stage, rows] = (
            down_share[stage, 2, rows].astype(F32) + down_in[stage, 0, rows].astype(F32)
        ).astype(BF16)
        cross_copy(at).start()

    def back_copy(at):
        p = index(at)
        return remote(
            finished.at[at[0], place_rows(at)],
            back.at[p],
            back_send.at[p],
            back_recv.at[p],
            {"sp": peer(at)},
        )

    def finish(at):
        stage, rows = at[0], place_rows(at)
        if at[1] == 0:
            half_copy(stage, 1).wait_recv()
        cross_copy(at).wait_recv()
        finished[stage, rows] = (
            down_share[stage, 3, rows].astype(F32)
            + down_in[stage, 1, rows].astype(F32)
            + down_pair_in[stage, rows].astype(F32)
        ).astype(BF16)
        if at != own:
            back_copy(at).start()

    def add_result(at):
        source = peer(at)
        if at == own:
            block = finished[at[0], place_rows(at)]
        else:
            back_copy(at).wait_recv()
            block = back[index(at)]
        weight = weight_cols[source][:, 0:1]
        stream[...] += weight * jnp.dot(
            select[source][:, 0:capacity], block, preferred_element_type=F32
        )

    def each(action, stage, place):
        if 0 <= stage < stages:
            action((stage, place))

    def each_remote(action, stage, place):
        if (stage, place) != own:
            each(action, stage, place)

    each_remote(direct, 0, 1)
    relay(own)
    direct((0, 0))
    each_remote(direct, 1, 1)
    for copy in local[1:]:
        copy.wait()
    for stage in range(stages):
        each_remote(relay, stage, 1)
        if stage == stages - 1:
            for early in range(stages - 2):
                cross((early, 1))
        expert_near(stage)
        relay((stage, 0))
        each(direct, stage + 1, 0)
        each(cross, stage - 1, 0)
        each_remote(direct, stage + 2, 1)
        each(finish, stage - 2, 0)
        expert_far(stage)
    for stage in range(stages - 2):
        finish((stage, 1))
    cross((stages - 1, 0))
    finish((stages - 2, 0))
    cross((stages - 2, 1))
    cross(own)
    add_result((0, 0))
    finish((stages - 1, 0))
    add_result((0, 1))
    finish((stages - 2, 1))
    for stage in range(1, stages - 1):
        add_result((stage, 0))
        add_result((stage, 1))
    finish(own)
    add_result(own)
    add_result((stages - 1, 0))
    out_ref[...] = stream[...].astype(BF16)

    for copy in halo_copies + to_partner + pair_copies + edge_copies + square_copies:
        copy.wait_send()
    for at in everyone:
        if at != own:
            row_copy(at).wait_send()
            scale_copy(at).wait_send()
            back_copy(at).wait_send()
        for kind in range(3):
            spread(at, kind).wait_send()
        cross_copy(at).wait_send()
    for stage in range(stages):
        half_copy(stage, 0).wait_send()
        half_copy(stage, 1).wait_send()


def fused(
    sp_count,
    in_gate,
    out_gate,
    values,
    conv_taps,
    doc_ids,
    residual,
    out_weight,
    norm_gain,
    routes,
    route_weights,
    expert_gate,
    expert_up,
    expert_down,
):
    channels, tokens = in_gate.shape
    model_width = residual.shape[1]
    width = model_width // 4
    capacity = 3 * tokens * routes.shape[1] // (2 * sp_count)
    slot_lanes = -(-2 * capacity // LANES) * LANES
    hidden = expert_gate.shape[2]
    stages = len(plan_stages(sp_count // 2))
    pair_rows = 2 * capacity
    vmem = pl.BlockSpec(memory_space=pltpu.VMEM)
    hbm = pl.BlockSpec(memory_space=pl.ANY)
    dma = pltpu.SemaphoreType.DMA
    return pl.pallas_call(
        functools.partial(layer_kernel, sp_count, capacity),
        out_shape=jax.ShapeDtypeStruct((tokens, width), BF16),
        in_specs=[vmem] * 5 + [hbm] + [vmem] * 4 + [hbm] * 3,
        out_specs=vmem,
        scratch_shapes=[
            pltpu.VMEM((hidden, model_width), BF16),
            pltpu.VMEM((hidden, model_width), BF16),
            pltpu.VMEM((hidden, model_width), BF16),
            pltpu.VMEM((model_width // LANES, LANES), F32),
            pltpu.VMEM((tokens, width), BF16),
            pltpu.VMEM((channels, tokens), BF16),
            pltpu.VMEM((16, channels), BF16),
            pltpu.VMEM((16, channels), BF16),
            pltpu.VMEM((1, tokens), jnp.int32),
            pltpu.VMEM((2, tokens, width), BF16),
            pltpu.VMEM((2, tokens, width), BF16),
            pltpu.VMEM((tokens, width), BF16),
            pltpu.VMEM((tokens, width), BF16),
            pltpu.VMEM((3, 16, width), BF16),
            pltpu.VMEM((3, 16, width), BF16),
            pltpu.VMEM((8, tokens), F32),
            pltpu.VMEM((3, 8, tokens), F32),
            pltpu.VMEM((sp_count, tokens), F32),
            pltpu.VMEM((sp_count, tokens, slot_lanes), BF16),
            pltpu.VMEM((sp_count, tokens, LANES), F32),
            pltpu.VMEM((sp_count, 8, slot_lanes), F32),
            pltpu.VMEM((sp_count, 8, slot_lanes), F32),
            pltpu.VMEM((tokens, width), F32),
            pltpu.VMEM((sp_count, capacity, width), BF16),
            pltpu.VMEM((stages, pair_rows, model_width), BF16),
            pltpu.VMEM((2, hidden, pair_rows), F32),
            pltpu.VMEM((2, hidden, pair_rows), F32),
            pltpu.VMEM((stages, 4, pair_rows, width), BF16),
            pltpu.VMEM((stages, 2, pair_rows, width), BF16),
            pltpu.VMEM((stages, pair_rows, width), BF16),
            pltpu.VMEM((stages, pair_rows, width), BF16),
            pltpu.VMEM((stages, pair_rows, width), BF16),
            pltpu.VMEM((sp_count, capacity, width), BF16),
            dma((2,)),
            dma((2,)),
            dma((4,)),
            dma((3,)),
            dma((3,)),
            dma((2,)),
            dma((2,)),
            dma((3,)),
            dma((3,)),
            dma((3,)),
            dma((3,)),
            dma((sp_count,)),
            dma((sp_count,)),
            dma((sp_count,)),
            dma((sp_count,)),
            dma((sp_count, 3)),
            dma((sp_count, 3)),
            dma((stages, 2)),
            dma((stages, 2)),
            dma((sp_count,)),
            dma((sp_count,)),
            dma((sp_count,)),
            dma((sp_count,)),
        ],
        compiler_params=pltpu.CompilerParams(
            collective_id=0, has_side_effects=True, vmem_limit_bytes=60 * 1024 * 1024
        ),
    )(
        in_gate,
        out_gate,
        values,
        conv_taps,
        doc_ids.reshape(1, tokens),
        residual,
        out_weight,
        norm_gain.reshape(model_width // LANES, LANES),
        routes.T,
        route_weights.T,
        expert_gate.transpose(0, 2, 1),
        expert_up.transpose(0, 2, 1),
        expert_down,
    )


def solution(mesh):
    placed = (
        P("tp", "sp"),
        P("tp", "sp"),
        P("tp", "sp"),
        P(None, "tp"),
        P("sp"),
        P("sp", None),
        P("tp", None),
        P(),
        P("sp", None),
        P("sp", None),
        P("sp", None, "tp"),
        P("sp", None, "tp"),
        P("sp", "tp", None),
    )
    sp_count, tp_count = mesh.shape["sp"], mesh.shape["tp"]
    planes = sp_count // 2
    paired = tp_count == 4 and sp_count % 4 == 0 and planes & (planes - 1) == 0
    body = functools.partial(fused, sp_count) if paired else shards
    return jax.shard_map(
        body, mesh=mesh, in_specs=placed, out_specs=P("sp", "tp"), check_vma=False
    )
```

```python
import functools

import jax
import jax.numpy as jnp
from jax import lax
from jax.experimental import pallas as pl
from jax.experimental.pallas import tpu as pltpu
from jax.sharding import PartitionSpec as P

EPSILON = 1e-06


def shifted(x, axis, by):
    count = lax.axis_size(axis)
    pairs = [(i, i + by) for i in range(count) if 0 <= i + by < count]
    return lax.ppermute(x, axis, pairs)


def shards(
    in_gate,
    out_gate,
    values,
    conv_taps,
    doc_ids,
    residual,
    out_weight,
    norm_gain,
    routes,
    route_weights,
    expert_gate,
    expert_up,
    expert_down,
):
    gated_in = (in_gate.astype(jnp.float32) * values.astype(jnp.float32)).astype(jnp.bfloat16)
    tail_rows, tail_docs = shifted((gated_in[:, -2:], doc_ids[-2:]), "sp", 1)
    extended = lax.optimization_barrier(jnp.concatenate([tail_rows, gated_in], axis=1)).astype(
        jnp.float32
    )
    docs_ext = jnp.concatenate([tail_docs, doc_ids])
    length = doc_ids.shape[0]
    near_mask = (docs_ext[1 : length + 1] == doc_ids).astype(jnp.float32)
    far_mask = (docs_ext[0:length] == doc_ids).astype(jnp.float32)
    tap_values = conv_taps.astype(jnp.float32)
    convolved = (
        tap_values[2][:, None] * extended[:, 2:]
        + tap_values[1][:, None] * extended[:, 1 : length + 1] * near_mask[None, :]
        + tap_values[0][:, None] * extended[:, 0:length] * far_mask[None, :]
    )
    mixed_rows = (out_gate.astype(jnp.float32) * convolved).astype(jnp.bfloat16)
    partial_value = lax.dot_general(
        mixed_rows, out_weight, (((0,), (0,)), ((), ())), preferred_element_type=jnp.float32
    )
    tp_count = lax.axis_size("tp")
    model_width = residual.shape[1]
    share_width = model_width // tp_count
    column = lax.axis_index("tp") * share_width
    stream = residual.astype(jnp.float32) + lax.psum(
        partial_value.astype(jnp.bfloat16), "tp"
    ).astype(jnp.float32)
    inv_rms = lax.rsqrt(jnp.mean(stream * stream, axis=1, keepdims=True) + EPSILON)
    normed = (stream * inv_rms * norm_gain.astype(jnp.float32)[None, :]).astype(jnp.bfloat16)
    stream_cols = lax.dynamic_slice_in_dim(stream, column, share_width, 1)
    own_cols = lax.dynamic_slice_in_dim(normed, column, share_width, 1)
    tokens = routes.shape[0]
    top_count = routes.shape[1]
    experts = lax.axis_size("sp")
    capacity = 3 * tokens * top_count // (2 * experts)
    chosen = routes.reshape(-1)
    hits_table = (chosen[:, None] == jnp.arange(experts, dtype=jnp.int32)[None, :]).astype(
        jnp.int32
    )
    earlier = jnp.cumsum(hits_table, axis=0) - hits_table
    ranked = jnp.sum(earlier * hits_table, axis=1)
    slot_index = chosen * capacity + ranked
    owners = jnp.arange(tokens * top_count, dtype=jnp.int32) // top_count
    source = jnp.zeros((experts * capacity,), jnp.int32).at[slot_index].set(owners)
    filled = jnp.zeros((experts * capacity,), jnp.bool_).at[slot_index].set(True)
    gate_weight = expert_gate[0]
    up_weight = expert_up[0]
    down_weight = expert_down[0]
    picked = jnp.where(
        filled[:, None], jnp.take(own_cols, source, axis=0), jnp.zeros((), jnp.bfloat16)
    ).reshape(experts, capacity, share_width)
    arrived = lax.all_to_all(picked, "sp", split_axis=0, concat_axis=0, tiled=True)
    slot_count = arrived.shape[1]
    row_block = arrived.reshape(-1, share_width)
    piece_cols = lax.all_gather(row_block, "tp", axis=1, tiled=True)
    gate_sum = jnp.dot(piece_cols, gate_weight, preferred_element_type=jnp.float32)
    up_sum = jnp.dot(piece_cols, up_weight, preferred_element_type=jnp.float32)
    hidden = (jax.nn.silu(gate_sum) * up_sum).astype(jnp.bfloat16)
    down_sum = jnp.dot(hidden, down_weight, preferred_element_type=jnp.float32)
    summed = lax.psum_scatter(down_sum.astype(jnp.bfloat16), "tp", scatter_dimension=1, tiled=True)
    returned = lax.all_to_all(
        summed.reshape(experts, slot_count, share_width),
        "sp",
        split_axis=0,
        concat_axis=0,
        tiled=True,
    )
    results = jnp.take(returned.reshape(experts * capacity, share_width), slot_index, axis=0)
    results = results.astype(jnp.float32).reshape(tokens, top_count, share_width)
    blended = jnp.sum(route_weights[:, :, None] * results, axis=1)
    return (stream_cols + blended).astype(jnp.bfloat16)

MESH = pl.DeviceIdType.MESH
F32 = jnp.float32
BF16 = jnp.bfloat16
LANES = 128


def xor_index(value, mask):
    bit = 1
    while bit <= mask:
        if mask & bit:
            value = value + bit - 2 * bit * lax.rem(lax.div(value, bit), 2)
        bit *= 2
    return value


def column_of(row, width):
    return jnp.transpose(jnp.broadcast_to(row, (LANES, row.shape[1])))[:, :width]


def across_rows(left, right):
    return lax.dot_general(left, right, (((1,), (1,)), ((), ())), preferred_element_type=F32)


def plan_stages(planes):
    far = [(mask, flip) for mask in range(planes // 2, planes) for flip in (0, 1)]
    near = [(0, 1)] + [(mask, flip) for mask in range(1, planes // 2) for flip in (0, 1)] + [(0, 0)]
    return list(zip(far, near))


FOUR_STAGE_ORDER = (
    "S10 S21 D01 D11",
    "L31 D00 S20 W",
    "N0 L01 D10 N1",
    "S30 L11 D21 L00",
    "G0 L10 D20 Q0",
    "R0 X00 G1 L21",
    "Q1 R1 D30 X10",
    "N2 L20 X01 N3",
    "F00 G2 L30 Q2",
    "R2 X20 X21 F10",
    "G3 Q3 R3 F01",
    "X30 X11 X31 F20",
    "A00 F21 F30 F11",
    "A10 A01 F31 A31",
    "A20 A21 E A11",
    "A30",
)


def plan_order(stages):
    if stages == 4:
        return " ".join(FOUR_STAGE_ORDER).split()
    blocks = [f"{stage}{place}" for stage in range(stages) for place in range(2)]
    order = ["S" + block for block in blocks[2:-1] if block != "11"]
    order += ["D" + block for block in blocks[:-1]] + ["L" + block for block in blocks] + ["W"]
    for stage in range(stages):
        order += [f"{step}{stage}" for step in "NGQR"]
        order += [f"X{stage}0", f"X{stage}1", f"F{stage}0", f"F{stage}1"]
    return order + ["E"] + ["A" + block for block in blocks]


def layer_kernel(
    sp_count,
    capacity,
    in_gate_ref,
    out_gate_ref,
    values_ref,
    taps_ref,
    docs_ref,
    residual_ref,
    out_weight_ref,
    gain_ref,
    routes_ref,
    weights_ref,
    gate_hbm,
    up_hbm,
    down_hbm,
    out_ref,
    gate_ref,
    up_ref,
    down_ref,
    gains,
    own_residual,
    gated,
    tail,
    halo,
    halo_docs,
    share,
    share_in,
    pair_sum,
    pair_in,
    edge,
    edge_in,
    squares,
    squares_in,
    keys,
    select,
    weight_cols,
    scales,
    scales_in,
    stream,
    picked,
    rows_ref,
    gate_part,
    up_part,
    hidden_ref,
    down_share,
    down_in,
    down_pair,
    down_pair_in,
    finished,
    back,
    halo_send,
    halo_recv,
    local_sem,
    share_send,
    share_recv,
    pair_send,
    pair_recv,
    edge_send,
    edge_recv,
    square_send,
    square_recv,
    scale_send,
    scale_recv,
    row_send,
    row_recv,
    spread_send,
    spread_recv,
    half_send,
    half_recv,
    cross_send,
    cross_recv,
    back_send,
    back_recv,
):
    me = lax.axis_index("sp")
    rank = lax.axis_index("tp")
    side, core = lax.div(rank, 2), lax.rem(rank, 2)
    plane, lane = lax.div(me, 2), lax.rem(me, 2)
    partner = 2 * side + 1 - core
    across = 2 * (1 - side) + core
    diagonal = 2 * (1 - side) + 1 - core
    channels, tokens = in_gate_ref.shape
    model_width = residual_ref.shape[1]
    width = stream.shape[1]
    half_width = width // 2
    places = plan_stages(sp_count // 2)
    stages = len(places)
    own = (stages - 1, 1)

    def cols(owner):
        return pl.ds(pl.multiple_of(owner * width, width), width)

    def chip_cols(which):
        return pl.ds(pl.multiple_of(which * 2 * width, 2 * width), 2 * width)

    def remote(src, dst, send, recv, device):
        return pltpu.make_async_remote_copy(
            src_ref=src, dst_ref=dst, send_sem=send, recv_sem=recv, device_id=device, device_id_type=MESH
        )

    def peer(at):
        mask, flip = places[at[0]][at[1]]
        return 2 * xor_index(plane, mask) + (1 - lane if flip else lane)

    local = [
        pltpu.make_async_copy(residual_ref.at[:, cols(rank)], own_residual, local_sem.at[0]),
        pltpu.make_async_copy(gate_hbm.at[0], gate_ref, local_sem.at[1]),
        pltpu.make_async_copy(up_hbm.at[0], up_ref, local_sem.at[2]),
        pltpu.make_async_copy(down_hbm.at[0], down_ref, local_sem.at[3]),
    ]
    for copy in local:
        copy.start()

    barrier = pltpu.get_barrier_semaphore()
    for step in range(1, sp_count):
        pl.semaphore_signal(
            barrier, inc=1, device_id={"sp": lax.rem(me + step, sp_count)}, device_id_type=MESH
        )
    for other in (partner, across, diagonal):
        pl.semaphore_signal(barrier, inc=1, device_id={"tp": other}, device_id_type=MESH)

    gains[...] = gain_ref[...].astype(F32)
    gated[...] = (in_gate_ref[...].astype(F32) * values_ref[...].astype(F32)).astype(BF16)
    head_rows = tail.shape[0]
    tail[...] = jnp.transpose(gated[:, tokens - LANES :].astype(F32))[LANES - head_rows :, :].astype(
        BF16
    )
    tap_rows = [taps_ref[k : k + 1, :].astype(F32) for k in range(3)]
    wide_taps = [
        jnp.concatenate([column_of(tap, LANES)] * (tokens // LANES), axis=1) for tap in tap_rows
    ]
    docs = jnp.broadcast_to(docs_ref[...], (8, tokens))
    token_row = lax.broadcasted_iota(jnp.int32, (8, tokens), 1)

    def same_document(by):
        alike = (pltpu.roll(docs, by, 1) == docs) & (token_row >= by)
        return jnp.where(alike, 1.0, 0.0)[0:1, :]

    main = gated[...].astype(F32)
    convolved = (
        wide_taps[2] * main
        + wide_taps[1] * pltpu.roll(main, 1, 1) * same_document(1)
        + wide_taps[0] * pltpu.roll(main, 2, 1) * same_document(2)
    )
    mixed = jnp.transpose(out_gate_ref[...].astype(F32) * convolved).astype(BF16)

    def projected(owner):
        return jnp.dot(mixed, out_weight_ref[:, cols(owner)], preferred_element_type=F32)

    halves = [pl.ds(k * half_width, half_width) for k in range(2)]
    to_partner = [
        remote(
            share.at[0, :, halves[k]],
            share_in.at[0, :, halves[k]],
            share_send.at[k],
            share_recv.at[k],
            {"tp": partner},
        )
        for k in range(2)
    ] + [remote(share.at[1], share_in.at[1], share_send.at[2], share_recv.at[2], {"tp": partner})]
    share[0] = projected(diagonal).astype(BF16)
    following = lax.rem(me + 1, sp_count)
    halo_copies = [
        remote(tail, halo, halo_send.at[0], halo_recv.at[0], {"sp": following}),
        remote(docs_ref, halo_docs, halo_send.at[1], halo_recv.at[1], {"sp": following}),
    ]
    middle = tokens // 2
    pair_parts = [
        (slice(0, 1), slice(head_rows, tokens)),
        (slice(1, 2), slice(middle, tokens)),
        (slice(0, 2), slice(0, head_rows)),
        (slice(1, 2), slice(head_rows, middle)),
    ]
    pair_copies = [
        remote(pair_sum.at[at], pair_in.at[at], pair_send.at[k], pair_recv.at[k], {"tp": across})
        for k, at in enumerate(pair_parts)
    ]

    def send_pair(k, extra=None):
        which, rows = pair_parts[k]
        for h in range(which.start, which.stop):
            columns = slice(h * half_width, (h + 1) * half_width)
            block = crossing[rows, columns] + share_in[0, rows, columns].astype(F32)
            if extra is not None:
                block = block + extra[:, columns]
            pair_sum[h, rows] = block.astype(BF16)
        pair_copies[k].start()

    pl.semaphore_wait(barrier, sp_count + 2)
    to_partner[0].start()
    to_partner[1].start()
    for copy in halo_copies:
        copy.start()
    crossing = projected(across)
    to_partner[0].wait_recv()
    send_pair(0)
    to_partner[1].wait_recv()
    send_pair(1)
    share[1] = projected(partner).astype(BF16)
    to_partner[2].start()
    stream[...] = projected(rank)

    for copy in halo_copies:
        copy.wait_recv()
    earlier = jnp.where(me > 0, halo[...].astype(F32), 0.0)
    old_docs = jnp.broadcast_to(halo_docs[...], (8, tokens))[:, tokens - LANES :]
    docs_ext = jnp.concatenate([old_docs, docs[:, :LANES]], axis=1)

    def carried_mask(by):
        alike = pltpu.roll(docs_ext, by, 1)[:, LANES:] == docs[:, :LANES]
        alike = alike & (token_row[:, :LANES] < by)
        return column_of(jnp.where(alike, 1.0, 0.0)[0:1, :], LANES)[0:head_rows, 0:1]

    carried = tap_rows[1] * pltpu.roll(earlier, 1, 0) * carried_mask(1) + tap_rows[0] * pltpu.roll(
        earlier, 2, 0
    ) * carried_mask(2)
    edge_mixed = jnp.transpose(out_gate_ref[:, 0:LANES].astype(F32))[0:head_rows, :] * carried
    edge_mixed = edge_mixed.astype(BF16)

    def edge_projected(owner):
        return jnp.dot(edge_mixed, out_weight_ref[:, cols(owner)], preferred_element_type=F32)

    edge_copies = [
        remote(edge.at[k], edge_in.at[k], edge_send.at[k], edge_recv.at[k], {"tp": partner})
        for k in range(2)
    ]
    for k, owner in enumerate((diagonal, partner)):
        edge[k] = edge_projected(owner).astype(BF16)
        edge_copies[k].start()
    crossing_edge = edge_projected(across)
    edge_copies[0].wait_recv()
    send_pair(2, crossing_edge + edge_in[0].astype(F32))
    send_pair(3)
    stream[0:head_rows, :] += edge_projected(rank)
    to_partner[2].wait_recv()
    local[0].wait()
    stream[...] += share_in[1].astype(F32) + own_residual[...].astype(F32)

    experts = lax.broadcasted_iota(jnp.int32, (sp_count, tokens), 0)
    hits = jnp.zeros((sp_count, tokens), F32)
    expert_weights = jnp.zeros((sp_count, tokens), F32)
    for k in range(routes_ref.shape[0]):
        named = routes_ref[k : k + 1, :] == experts
        hits = jnp.where(named, 1.0, hits)
        expert_weights = jnp.where(named, weights_ref[k : k + 1, :], expert_weights)
    before = lax.broadcasted_iota(jnp.int32, (tokens, tokens), 0) < lax.broadcasted_iota(
        jnp.int32, (tokens, tokens), 1
    )
    ranks = jnp.dot(
        hits.astype(BF16), jnp.where(before, 1.0, 0.0).astype(BF16), preferred_element_type=F32
    )
    key_rows = jnp.where(hits > 0.5, ranks, -1.0)
    keys[...] = key_rows
    slot_lanes = select.shape[2]
    lanes = lax.broadcasted_iota(jnp.int32, (tokens, slot_lanes), 1)
    slots = jnp.where(lanes < capacity, lanes, lanes - capacity)
    slots = jnp.where(lanes < 2 * capacity, slots, -2).astype(F32)
    for expert_index in range(sp_count):
        one = slice(expert_index, expert_index + 1)
        key_cols = jnp.concatenate(
            [column_of(key_rows[one, :], LANES)] * (slot_lanes // LANES), axis=1
        )
        select[expert_index] = jnp.where(key_cols == slots, 1.0, 0.0).astype(BF16)
        weight_cols[expert_index] = column_of(expert_weights[one, :], LANES)

    per_rank = width // LANES
    gain = jnp.concatenate(
        [gains[pl.ds(rank * per_rank + k, 1), :] for k in range(per_rank)], axis=1
    )
    edge_copies[1].wait_recv()
    stream[0:head_rows, :] += edge_in[1].astype(F32)

    def scaled_half(k):
        for part in ((0, 2), (1, 3))[k]:
            pair_copies[part].wait_recv()
        total = stream[:, halves[k]] + pair_in[k].astype(F32)
        stream[:, halves[k]] = total
        own_gain = gain[:, k * half_width : (k + 1) * half_width]
        return (total * own_gain).astype(BF16), jnp.sum(total * total, axis=1, keepdims=True)

    def place_rows(at):
        return pl.ds(at[1] * capacity, capacity)

    slot_rows = lax.broadcasted_iota(jnp.int32, (capacity, tokens), 0).astype(F32)

    def index(at):
        return 2 * at[0] + at[1]

    def pick(at, k):
        chosen = jnp.where(keys[pl.ds(peer(at), 1), :] == slot_rows, 1.0, 0.0).astype(BF16)
        return jnp.dot(chosen, scaled[k], preferred_element_type=F32).astype(BF16)

    def row_copy(at, k):
        p = index(at)
        return remote(
            picked.at[p, k],
            rows_ref.at[at[0], rank, k, place_rows(at)],
            row_send.at[p, k],
            row_recv.at[p, k],
            {"sp": peer(at)},
        )

    def spread(at, kind):
        owner, device = ((rank, across), (rank, partner), (across, partner))[kind]
        block = rows_ref.at[at[0], owner, :, place_rows(at)]
        p = index(at)
        return remote(
            block, block, spread_send.at[p, kind], spread_recv.at[p, kind], {"tp": device}
        )

    def spread_arrival(at, kind):
        owner = (across, partner, diagonal)[kind]
        block = rows_ref.at[at[0], owner, :, place_rows(at)]
        p = index(at)
        return remote(
            block, block, spread_send.at[p, kind], spread_recv.at[p, kind], {"tp": partner}
        )

    def fill_rows(at, k):
        if at == own:
            rows_ref[at[0], rank, k, place_rows(at)] = pick(at, k)
        else:
            picked[index(at), k] = pick(at, k)

    def send_rows(at, k):
        if at != own:
            row_copy(at, k).start()

    everyone = [(stage, place) for stage in range(stages) for place in range(2)]
    send_order = [(0, 1), own, (0, 0)] + [
        at for stage in range(1, stages) for at in ((stage, 1), (stage, 0)) if at != own
    ]
    first = send_order[:4]
    scaled, half_squares = [], []
    for k in range(2):
        block, square = scaled_half(k)
        scaled.append(block)
        half_squares.append(square)
        if k == 0:
            for at in first:
                fill_rows(at, k)
                send_rows(at, k)

    own_square = half_squares[0] + half_squares[1]
    squares[...] = jnp.transpose(jnp.broadcast_to(own_square, (tokens, LANES)))[0:8, :]
    square_copies = [
        remote(
            squares, squares_in.at[k], square_send.at[k], square_recv.at[k], {"tp": other}
        )
        for k, other in enumerate((partner, across, diagonal))
    ]
    for copy in square_copies:
        copy.start()
    for at in first:
        fill_rows(at, 1)
        send_rows(at, 1)
        if at == own:
            spread(at, 0).start()
            spread(at, 1).start()

    def scale_copy(at):
        p = index(at)
        return remote(
            scales.at[p], scales_in.at[p], scale_send.at[p], scale_recv.at[p], {"sp": peer(at)}
        )

    def send_scales():
        for copy in square_copies:
            copy.wait_recv()
        all_squares = squares[...] + squares_in[0] + squares_in[1] + squares_in[2]
        inv_rms = column_of(lax.rsqrt(all_squares / model_width + EPSILON)[0:1, :], LANES)
        inv_cols = jnp.concatenate([inv_rms] * (slot_lanes // LANES), axis=1)
        for at in send_order:
            row = jnp.sum(select[peer(at)].astype(F32) * inv_cols, axis=0, keepdims=True)
            if at == own:
                scales_in[index(at)] = jnp.broadcast_to(row, scales.shape[1:])
            else:
                scales[index(at)] = jnp.broadcast_to(row, scales.shape[1:])
                scale_copy(at).start()

    def direct(at):
        row_copy(at, 0).wait_recv()
        row_copy(at, 1).wait_recv()
        spread(at, 0).start()
        spread(at, 1).start()

    def relay(at):
        spread_arrival(at, 0).wait_recv()
        spread(at, 2).start()

    def half_copy(stage, k):
        return remote(
            down_share.at[stage, k],
            down_in.at[stage, k],
            half_send.at[stage, k],
            half_recv.at[stage, k],
            {"tp": partner},
        )

    arrived = set()

    def half_arrival(stage, k):
        if (stage, k) not in arrived:
            arrived.add((stage, k))
            half_copy(stage, k).wait_recv()

    def chip_rows(stage, which):
        pieces = [rows_ref[stage, 2 * which + k // 2, k % 2] for k in range(4)]
        return jnp.concatenate(pieces, axis=1)

    def expert_near(stage):
        for place in range(2):
            spread_arrival((stage, place), 1).wait_recv()
        block = chip_rows(stage, side)
        gate_part[stage % 2] = across_rows(gate_ref[:, chip_cols(side)], block)
        up_part[stage % 2] = across_rows(up_ref[:, chip_cols(side)], block)

    def expert_far(stage):
        for place in range(2):
            spread_arrival((stage, place), 2).wait_recv()
            if (stage, place) != own:
                scale_copy((stage, place)).wait_recv()
        block = chip_rows(stage, 1 - side)
        scale_lane = lax.broadcasted_iota(jnp.int32, scales.shape[1:], 1)
        scale = jnp.where(scale_lane < capacity, scales_in[2 * stage], scales_in[2 * stage + 1])
        scale = scale[0:1, 0 : 2 * capacity]
        gate_sum = gate_part[stage % 2] + across_rows(gate_ref[:, chip_cols(1 - side)], block)
        up_sum = up_part[stage % 2] + across_rows(up_ref[:, chip_cols(1 - side)], block)
        gate_sum = gate_sum * scale
        up_sum = up_sum * scale
        hidden = gate_sum / (1.0 + jnp.exp(-gate_sum)) * up_sum
        hidden_ref[stage % 2] = jnp.transpose(hidden).astype(BF16)

    def expert_down(stage, k):
        owner = (diagonal, partner, across, rank)[k]
        down_share[stage, k] = jnp.dot(
            hidden_ref[stage % 2], down_ref[:, cols(owner)], preferred_element_type=F32
        ).astype(BF16)
        if k < 2:
            half_copy(stage, k).start()

    def cross_copy(at):
        return remote(
            down_pair.at[at[0], place_rows(at)],
            down_pair_in.at[at[0], place_rows(at)],
            cross_send.at[index(at)],
            cross_recv.at[index(at)],
            {"tp": across},
        )

    def cross(at):
        stage, rows = at[0], place_rows(at)
        half_arrival(stage, 0)
        down_pair[stage, rows] = (
            down_share[stage, 2, rows].astype(F32) + down_in[stage, 0, rows].astype(F32)
        ).astype(BF16)
        cross_copy(at).start()

    def back_copy(at):
        p = index(at)
        return remote(
            finished.at[at[0], place_rows(at)],
            back.at[p],
            back_send.at[p],
            back_recv.at[p],
            {"sp": peer(at)},
        )

    def finish(at):
        stage, rows = at[0], place_rows(at)
        half_arrival(stage, 1)
        cross_copy(at).wait_recv()
        finished[stage, rows] = (
            down_share[stage, 3, rows].astype(F32)
            + down_in[stage, 1, rows].astype(F32)
            + down_pair_in[stage, rows].astype(F32)
        ).astype(BF16)
        if at != own:
            back_copy(at).start()

    def add_result(at):
        source = peer(at)
        if at == own:
            block = finished[at[0], place_rows(at)]
        else:
            back_copy(at).wait_recv()
            block = back[index(at)]
        weight = weight_cols[source][:, 0:1]
        stream[...] += weight * jnp.dot(
            select[source][:, 0:capacity], block, preferred_element_type=F32
        )

    send_scales()
    def send_later(at):
        for k in range(2):
            fill_rows(at, k)
            send_rows(at, k)

    def weights_here():
        for copy in local[1:]:
            copy.wait()

    def sends_done():
        for copy in halo_copies + to_partner + pair_copies + edge_copies + square_copies:
            copy.wait_send()
        for at in everyone:
            if at != own:
                row_copy(at, 0).wait_send()
                row_copy(at, 1).wait_send()
                scale_copy(at).wait_send()
            for kind in range(3):
                spread(at, kind).wait_send()
            cross_copy(at).wait_send()
        for stage in range(stages):
            half_copy(stage, 0).wait_send()
            half_copy(stage, 1).wait_send()

    on_blocks = {"S": send_later, "D": direct, "L": relay, "X": cross, "F": finish, "A": add_result}
    on_stages = {
        "N": expert_near,
        "G": expert_far,
        "Q": lambda stage: [expert_down(stage, k) for k in (0, 1)],
        "R": lambda stage: [expert_down(stage, k) for k in (2, 3)],
    }
    for step in plan_order(stages):
        if step == "W":
            weights_here()
        elif step == "E":
            sends_done()
        elif step[0] in on_stages:
            on_stages[step[0]](int(step[1]))
        else:
            on_blocks[step[0]]((int(step[1]), int(step[2])))
    out_ref[...] = stream[...].astype(BF16)

    for at in everyone:
        if at != own:
            back_copy(at).wait_send()


def fused(
    sp_count,
    in_gate,
    out_gate,
    values,
    conv_taps,
    doc_ids,
    residual,
    out_weight,
    norm_gain,
    routes,
    route_weights,
    expert_gate,
    expert_up,
    expert_down,
):
    channels, tokens = in_gate.shape
    model_width = residual.shape[1]
    width = model_width // 4
    capacity = 3 * tokens * routes.shape[1] // (2 * sp_count)
    slot_lanes = -(-2 * capacity // LANES) * LANES
    hidden = expert_gate.shape[2]
    stages = len(plan_stages(sp_count // 2))
    pair_rows = 2 * capacity
    vmem = pl.BlockSpec(memory_space=pltpu.VMEM)
    hbm = pl.BlockSpec(memory_space=pl.ANY)
    dma = pltpu.SemaphoreType.DMA
    return pl.pallas_call(
        functools.partial(layer_kernel, sp_count, capacity),
        out_shape=jax.ShapeDtypeStruct((tokens, width), BF16),
        in_specs=[vmem] * 5 + [hbm] + [vmem] * 4 + [hbm] * 3,
        out_specs=vmem,
        scratch_shapes=[
            pltpu.VMEM((hidden, model_width), BF16),
            pltpu.VMEM((hidden, model_width), BF16),
            pltpu.VMEM((hidden, model_width), BF16),
            pltpu.VMEM((model_width // LANES, LANES), F32),
            pltpu.VMEM((tokens, width), BF16),
            pltpu.VMEM((channels, tokens), BF16),
            pltpu.VMEM((16, channels), BF16),
            pltpu.VMEM((16, channels), BF16),
            pltpu.VMEM((1, tokens), jnp.int32),
            pltpu.VMEM((2, tokens, width), BF16),
            pltpu.VMEM((2, tokens, width), BF16),
            pltpu.VMEM((2, tokens, width // 2), BF16),
            pltpu.VMEM((2, tokens, width // 2), BF16),
            pltpu.VMEM((2, 16, width), BF16),
            pltpu.VMEM((2, 16, width), BF16),
            pltpu.VMEM((8, tokens), F32),
            pltpu.VMEM((3, 8, tokens), F32),
            pltpu.VMEM((sp_count, tokens), F32),
            pltpu.VMEM((sp_count, tokens, slot_lanes), BF16),
            pltpu.VMEM((sp_count, tokens, LANES), F32),
            pltpu.VMEM((sp_count, 8, slot_lanes), F32),
            pltpu.VMEM((sp_count, 8, slot_lanes), F32),
            pltpu.VMEM((tokens, width), F32),
            pltpu.VMEM((sp_count, 2, capacity, width // 2), BF16),
            pltpu.VMEM((stages, 4, 2, pair_rows, width // 2), BF16),
            pltpu.VMEM((2, hidden, pair_rows), F32),
            pltpu.VMEM((2, hidden, pair_rows), F32),
            pltpu.VMEM((2, pair_rows, hidden), BF16),
            pltpu.VMEM((stages, 4, pair_rows, width), BF16),
            pltpu.VMEM((stages, 2, pair_rows, width), BF16),
            pltpu.VMEM((stages, pair_rows, width), BF16),
            pltpu.VMEM((stages, pair_rows, width), BF16),
            pltpu.VMEM((stages, pair_rows, width), BF16),
            pltpu.VMEM((sp_count, capacity, width), BF16),
            dma((2,)),
            dma((2,)),
            dma((4,)),
            dma((3,)),
            dma((3,)),
            dma((4,)),
            dma((4,)),
            dma((2,)),
            dma((2,)),
            dma((3,)),
            dma((3,)),
            dma((sp_count,)),
            dma((sp_count,)),
            dma((sp_count, 2)),
            dma((sp_count, 2)),
            dma((sp_count, 3)),
            dma((sp_count, 3)),
            dma((stages, 2)),
            dma((stages, 2)),
            dma((sp_count,)),
            dma((sp_count,)),
            dma((sp_count,)),
            dma((sp_count,)),
        ],
        compiler_params=pltpu.CompilerParams(
            collective_id=0, has_side_effects=True, vmem_limit_bytes=60 * 1024 * 1024
        ),
    )(
        in_gate,
        out_gate,
        values,
        conv_taps,
        doc_ids.reshape(1, tokens),
        residual,
        out_weight,
        norm_gain.reshape(model_width // LANES, LANES),
        routes.T,
        route_weights.T,
        expert_gate.transpose(0, 2, 1),
        expert_up.transpose(0, 2, 1),
        expert_down,
    )


def solution(mesh):
    placed = (
        P("tp", "sp"),
        P("tp", "sp"),
        P("tp", "sp"),
        P(None, "tp"),
        P("sp"),
        P("sp", None),
        P("tp", None),
        P(),
        P("sp", None),
        P("sp", None),
        P("sp", None, "tp"),
        P("sp", None, "tp"),
        P("sp", "tp", None),
    )
    sp_count, tp_count = mesh.shape["sp"], mesh.shape["tp"]
    planes = sp_count // 2
    paired = tp_count == 4 and sp_count % 4 == 0 and planes & (planes - 1) == 0
    body = functools.partial(fused, sp_count) if paired else shards
    return jax.shard_map(
        body, mesh=mesh, in_specs=placed, out_specs=P("sp", "tp"), check_vma=False
    )
```

```python
import functools

import jax
import jax.numpy as jnp
from jax import lax
from jax.experimental import pallas as pl
from jax.experimental.pallas import tpu as pltpu
from jax.sharding import PartitionSpec as P

EPSILON = 1e-06


def shifted(x, axis, by):
    count = lax.axis_size(axis)
    pairs = [(i, i + by) for i in range(count) if 0 <= i + by < count]
    return lax.ppermute(x, axis, pairs)


def shards(
    in_gate,
    out_gate,
    values,
    conv_taps,
    doc_ids,
    residual,
    out_weight,
    norm_gain,
    routes,
    route_weights,
    expert_gate,
    expert_up,
    expert_down,
):
    gated_in = (in_gate.astype(jnp.float32) * values.astype(jnp.float32)).astype(jnp.bfloat16)
    tail_rows, tail_docs = shifted((gated_in[:, -2:], doc_ids[-2:]), "sp", 1)
    extended = lax.optimization_barrier(jnp.concatenate([tail_rows, gated_in], axis=1)).astype(
        jnp.float32
    )
    docs_ext = jnp.concatenate([tail_docs, doc_ids])
    length = doc_ids.shape[0]
    near_mask = (docs_ext[1 : length + 1] == doc_ids).astype(jnp.float32)
    far_mask = (docs_ext[0:length] == doc_ids).astype(jnp.float32)
    tap_values = conv_taps.astype(jnp.float32)
    convolved = (
        tap_values[2][:, None] * extended[:, 2:]
        + tap_values[1][:, None] * extended[:, 1 : length + 1] * near_mask[None, :]
        + tap_values[0][:, None] * extended[:, 0:length] * far_mask[None, :]
    )
    mixed_rows = (out_gate.astype(jnp.float32) * convolved).astype(jnp.bfloat16)
    partial_value = lax.dot_general(
        mixed_rows, out_weight, (((0,), (0,)), ((), ())), preferred_element_type=jnp.float32
    )
    tp_count = lax.axis_size("tp")
    model_width = residual.shape[1]
    share_width = model_width // tp_count
    column = lax.axis_index("tp") * share_width
    stream = residual.astype(jnp.float32) + lax.psum(
        partial_value.astype(jnp.bfloat16), "tp"
    ).astype(jnp.float32)
    inv_rms = lax.rsqrt(jnp.mean(stream * stream, axis=1, keepdims=True) + EPSILON)
    normed = (stream * inv_rms * norm_gain.astype(jnp.float32)[None, :]).astype(jnp.bfloat16)
    stream_cols = lax.dynamic_slice_in_dim(stream, column, share_width, 1)
    own_cols = lax.dynamic_slice_in_dim(normed, column, share_width, 1)
    tokens = routes.shape[0]
    top_count = routes.shape[1]
    experts = lax.axis_size("sp")
    capacity = 3 * tokens * top_count // (2 * experts)
    chosen = routes.reshape(-1)
    hits_table = (chosen[:, None] == jnp.arange(experts, dtype=jnp.int32)[None, :]).astype(
        jnp.int32
    )
    earlier = jnp.cumsum(hits_table, axis=0) - hits_table
    ranked = jnp.sum(earlier * hits_table, axis=1)
    slot_index = chosen * capacity + ranked
    owners = jnp.arange(tokens * top_count, dtype=jnp.int32) // top_count
    source = jnp.zeros((experts * capacity,), jnp.int32).at[slot_index].set(owners)
    filled = jnp.zeros((experts * capacity,), jnp.bool_).at[slot_index].set(True)
    gate_weight = expert_gate[0]
    up_weight = expert_up[0]
    down_weight = expert_down[0]
    picked = jnp.where(
        filled[:, None], jnp.take(own_cols, source, axis=0), jnp.zeros((), jnp.bfloat16)
    ).reshape(experts, capacity, share_width)
    arrived = lax.all_to_all(picked, "sp", split_axis=0, concat_axis=0, tiled=True)
    slot_count = arrived.shape[1]
    row_block = arrived.reshape(-1, share_width)
    piece_cols = lax.all_gather(row_block, "tp", axis=1, tiled=True)
    gate_sum = jnp.dot(piece_cols, gate_weight, preferred_element_type=jnp.float32)
    up_sum = jnp.dot(piece_cols, up_weight, preferred_element_type=jnp.float32)
    hidden = (jax.nn.silu(gate_sum) * up_sum).astype(jnp.bfloat16)
    down_sum = jnp.dot(hidden, down_weight, preferred_element_type=jnp.float32)
    summed = lax.psum_scatter(down_sum.astype(jnp.bfloat16), "tp", scatter_dimension=1, tiled=True)
    returned = lax.all_to_all(
        summed.reshape(experts, slot_count, share_width),
        "sp",
        split_axis=0,
        concat_axis=0,
        tiled=True,
    )
    results = jnp.take(returned.reshape(experts * capacity, share_width), slot_index, axis=0)
    results = results.astype(jnp.float32).reshape(tokens, top_count, share_width)
    blended = jnp.sum(route_weights[:, :, None] * results, axis=1)
    return (stream_cols + blended).astype(jnp.bfloat16)

MESH = pl.DeviceIdType.MESH
F32 = jnp.float32
BF16 = jnp.bfloat16
LANES = 128


def xor_index(value, mask):
    bit = 1
    while bit <= mask:
        if mask & bit:
            value = value + bit - 2 * bit * lax.rem(lax.div(value, bit), 2)
        bit *= 2
    return value


def column_of(row, width):
    return jnp.transpose(jnp.broadcast_to(row, (LANES, row.shape[1])))[:, :width]


def across_rows(left, right):
    return lax.dot_general(left, right, (((1,), (1,)), ((), ())), preferred_element_type=F32)


def plan_stages(planes):
    far = [
        (mask, (flip + mask // (planes - 1)) % 2)
        for mask in range(planes // 2, planes)
        for flip in (0, 1)
    ]
    near = [(0, 1)] + [(mask, flip) for mask in range(1, planes // 2) for flip in (0, 1)] + [(0, 0)]
    return list(zip(far, near))


FOUR_STAGE_ORDER = (
    "S10 S21 D01 D11",
    "L31 D00 S20 W",
    "N0 L01 D10 N1",
    "S30 L11 D21 L00",
    "G0 L10 D20 Q0",
    "R0 X00 G1 L21",
    "Q1 R1 D30 X10",
    "N2 L20 X01 N3",
    "F00 G2 L30 Q2",
    "R2 X20 X11 F10",
    "G3 Q3 R3 F01",
    "X30 X21 X31 F20",
    "A00 F11 F30 F21",
    "A10 A01 F31 A31",
    "A20 A11 E A30",
    "A21",
)


def plan_order(stages):
    if stages == 4:
        return " ".join(FOUR_STAGE_ORDER).split()
    blocks = [f"{stage}{place}" for stage in range(stages) for place in range(2)]
    order = ["S" + block for block in blocks[2:-1] if block != "11"]
    order += ["D" + block for block in blocks[:-1]] + ["L" + block for block in blocks] + ["W"]
    for stage in range(stages):
        order += [f"{step}{stage}" for step in "NGQR"]
        order += [f"X{stage}0", f"X{stage}1", f"F{stage}0", f"F{stage}1"]
    return order + ["E"] + ["A" + block for block in blocks]


def layer_kernel(
    sp_count,
    capacity,
    in_gate_ref,
    out_gate_ref,
    values_ref,
    taps_ref,
    docs_ref,
    residual_ref,
    out_weight_ref,
    gain_ref,
    routes_ref,
    weights_ref,
    gate_hbm,
    up_hbm,
    down_hbm,
    out_ref,
    gate_ref,
    up_ref,
    down_ref,
    gains,
    own_residual,
    gated,
    tail,
    halo,
    halo_docs,
    share,
    share_in,
    pair_sum,
    pair_in,
    edge,
    edge_in,
    squares,
    squares_in,
    keys,
    select,
    weight_cols,
    scales,
    scales_in,
    stream,
    picked,
    rows_ref,
    gate_part,
    up_part,
    hidden_ref,
    down_share,
    down_in,
    down_pair,
    down_pair_in,
    finished,
    back,
    halo_send,
    halo_recv,
    local_sem,
    share_send,
    share_recv,
    pair_send,
    pair_recv,
    edge_send,
    edge_recv,
    square_send,
    square_recv,
    scale_send,
    scale_recv,
    row_send,
    row_recv,
    spread_send,
    spread_recv,
    half_send,
    half_recv,
    cross_send,
    cross_recv,
    back_send,
    back_recv,
):
    me = lax.axis_index("sp")
    rank = lax.axis_index("tp")
    side, core = lax.div(rank, 2), lax.rem(rank, 2)
    plane, lane = lax.div(me, 2), lax.rem(me, 2)
    partner = 2 * side + 1 - core
    across = 2 * (1 - side) + core
    diagonal = 2 * (1 - side) + 1 - core
    channels, tokens = in_gate_ref.shape
    model_width = residual_ref.shape[1]
    width = stream.shape[1]
    half_width = width // 2
    places = plan_stages(sp_count // 2)
    stages = len(places)
    own = (stages - 1, 1)

    def cols(owner):
        return pl.ds(pl.multiple_of(owner * width, width), width)

    def chip_cols(which):
        return pl.ds(pl.multiple_of(which * 2 * width, 2 * width), 2 * width)

    def remote(src, dst, send, recv, device):
        return pltpu.make_async_remote_copy(
            src_ref=src, dst_ref=dst, send_sem=send, recv_sem=recv, device_id=device, device_id_type=MESH
        )

    def peer(at):
        mask, flip = places[at[0]][at[1]]
        return 2 * xor_index(plane, mask) + (1 - lane if flip else lane)

    local = [
        pltpu.make_async_copy(residual_ref.at[:, cols(rank)], own_residual, local_sem.at[0]),
        pltpu.make_async_copy(gate_hbm.at[0], gate_ref, local_sem.at[1]),
        pltpu.make_async_copy(up_hbm.at[0], up_ref, local_sem.at[2]),
        pltpu.make_async_copy(down_hbm.at[0], down_ref, local_sem.at[3]),
    ]
    for copy in local:
        copy.start()

    barrier = pltpu.get_barrier_semaphore()
    for step in range(1, sp_count):
        pl.semaphore_signal(
            barrier, inc=1, device_id={"sp": lax.rem(me + step, sp_count)}, device_id_type=MESH
        )
    for other in (partner, across, diagonal):
        pl.semaphore_signal(barrier, inc=1, device_id={"tp": other}, device_id_type=MESH)

    gains[...] = gain_ref[...].astype(F32)
    gated[...] = (in_gate_ref[...].astype(F32) * values_ref[...].astype(F32)).astype(BF16)
    head_rows = tail.shape[0]
    tail[...] = jnp.transpose(gated[:, tokens - LANES :].astype(F32))[LANES - head_rows :, :].astype(
        BF16
    )
    tap_rows = [taps_ref[k : k + 1, :].astype(F32) for k in range(3)]
    wide_taps = [
        jnp.concatenate([column_of(tap, LANES)] * (tokens // LANES), axis=1) for tap in tap_rows
    ]
    docs = jnp.broadcast_to(docs_ref[...], (8, tokens))
    token_row = lax.broadcasted_iota(jnp.int32, (8, tokens), 1)

    def same_document(by):
        alike = (pltpu.roll(docs, by, 1) == docs) & (token_row >= by)
        return jnp.where(alike, 1.0, 0.0)[0:1, :]

    main = gated[...].astype(F32)
    convolved = (
        wide_taps[2] * main
        + wide_taps[1] * pltpu.roll(main, 1, 1) * same_document(1)
        + wide_taps[0] * pltpu.roll(main, 2, 1) * same_document(2)
    )
    mixed = jnp.transpose(out_gate_ref[...].astype(F32) * convolved).astype(BF16)

    def projected(owner):
        return jnp.dot(mixed, out_weight_ref[:, cols(owner)], preferred_element_type=F32)

    halves = [pl.ds(k * half_width, half_width) for k in range(2)]
    to_partner = [
        remote(
            share.at[0, :, halves[k]],
            share_in.at[0, :, halves[k]],
            share_send.at[k],
            share_recv.at[k],
            {"tp": partner},
        )
        for k in range(2)
    ] + [remote(share.at[1], share_in.at[1], share_send.at[2], share_recv.at[2], {"tp": partner})]
    share[0] = projected(diagonal).astype(BF16)
    following = lax.rem(me + 1, sp_count)
    halo_copies = [
        remote(tail, halo, halo_send.at[0], halo_recv.at[0], {"sp": following}),
        remote(docs_ref, halo_docs, halo_send.at[1], halo_recv.at[1], {"sp": following}),
    ]
    middle = tokens // 2
    pair_parts = [
        (slice(0, 1), slice(head_rows, tokens)),
        (slice(1, 2), slice(middle, tokens)),
        (slice(0, 2), slice(0, head_rows)),
        (slice(1, 2), slice(head_rows, middle)),
    ]
    pair_copies = [
        remote(pair_sum.at[at], pair_in.at[at], pair_send.at[k], pair_recv.at[k], {"tp": across})
        for k, at in enumerate(pair_parts)
    ]

    def send_pair(k, extra=None):
        which, rows = pair_parts[k]
        for h in range(which.start, which.stop):
            columns = slice(h * half_width, (h + 1) * half_width)
            block = crossing[rows, columns] + share_in[0, rows, columns].astype(F32)
            if extra is not None:
                block = block + extra[:, columns]
            pair_sum[h, rows] = block.astype(BF16)
        pair_copies[k].start()

    pl.semaphore_wait(barrier, sp_count + 2)
    to_partner[0].start()
    to_partner[1].start()
    for copy in halo_copies:
        copy.start()
    crossing = projected(across)
    to_partner[0].wait_recv()
    send_pair(0)
    to_partner[1].wait_recv()
    send_pair(1)
    share[1] = projected(partner).astype(BF16)
    to_partner[2].start()
    stream[...] = projected(rank)

    for copy in halo_copies:
        copy.wait_recv()
    earlier = jnp.where(me > 0, halo[...].astype(F32), 0.0)
    old_docs = jnp.broadcast_to(halo_docs[...], (8, tokens))[:, tokens - LANES :]
    docs_ext = jnp.concatenate([old_docs, docs[:, :LANES]], axis=1)

    def carried_mask(by):
        alike = pltpu.roll(docs_ext, by, 1)[:, LANES:] == docs[:, :LANES]
        alike = alike & (token_row[:, :LANES] < by)
        return column_of(jnp.where(alike, 1.0, 0.0)[0:1, :], LANES)[0:head_rows, 0:1]

    carried = tap_rows[1] * pltpu.roll(earlier, 1, 0) * carried_mask(1) + tap_rows[0] * pltpu.roll(
        earlier, 2, 0
    ) * carried_mask(2)
    edge_mixed = jnp.transpose(out_gate_ref[:, 0:LANES].astype(F32))[0:head_rows, :] * carried
    edge_mixed = edge_mixed.astype(BF16)

    def edge_projected(owner):
        return jnp.dot(edge_mixed, out_weight_ref[:, cols(owner)], preferred_element_type=F32)

    edge_copies = [
        remote(edge.at[k], edge_in.at[k], edge_send.at[k], edge_recv.at[k], {"tp": partner})
        for k in range(2)
    ]
    for k, owner in enumerate((diagonal, partner)):
        edge[k] = edge_projected(owner).astype(BF16)
        edge_copies[k].start()
    crossing_edge = edge_projected(across)
    edge_copies[0].wait_recv()
    send_pair(2, crossing_edge + edge_in[0].astype(F32))
    send_pair(3)
    stream[0:head_rows, :] += edge_projected(rank)
    to_partner[2].wait_recv()
    local[0].wait()
    stream[...] += share_in[1].astype(F32) + own_residual[...].astype(F32)

    experts = lax.broadcasted_iota(jnp.int32, (sp_count, tokens), 0)
    hits = jnp.zeros((sp_count, tokens), F32)
    expert_weights = jnp.zeros((sp_count, tokens), F32)
    for k in range(routes_ref.shape[0]):
        named = routes_ref[k : k + 1, :] == experts
        hits = jnp.where(named, 1.0, hits)
        expert_weights = jnp.where(named, weights_ref[k : k + 1, :], expert_weights)
    before = lax.broadcasted_iota(jnp.int32, (tokens, tokens), 0) < lax.broadcasted_iota(
        jnp.int32, (tokens, tokens), 1
    )
    ranks = jnp.dot(
        hits.astype(BF16), jnp.where(before, 1.0, 0.0).astype(BF16), preferred_element_type=F32
    )
    key_rows = jnp.where(hits > 0.5, ranks, -1.0)
    keys[...] = key_rows
    slot_lanes = select.shape[2]
    lanes = lax.broadcasted_iota(jnp.int32, (tokens, slot_lanes), 1)
    slots = jnp.where(lanes < capacity, lanes, lanes - capacity)
    slots = jnp.where(lanes < 2 * capacity, slots, -2).astype(F32)
    for expert_index in range(sp_count):
        one = slice(expert_index, expert_index + 1)
        key_cols = jnp.concatenate(
            [column_of(key_rows[one, :], LANES)] * (slot_lanes // LANES), axis=1
        )
        select[expert_index] = jnp.where(key_cols == slots, 1.0, 0.0).astype(BF16)
        weight_cols[expert_index] = column_of(expert_weights[one, :], LANES)

    per_rank = width // LANES
    gain = jnp.concatenate(
        [gains[pl.ds(rank * per_rank + k, 1), :] for k in range(per_rank)], axis=1
    )
    edge_copies[1].wait_recv()
    stream[0:head_rows, :] += edge_in[1].astype(F32)

    def scaled_half(k):
        for part in ((0, 2), (1, 3))[k]:
            pair_copies[part].wait_recv()
        total = stream[:, halves[k]] + pair_in[k].astype(F32)
        stream[:, halves[k]] = total
        own_gain = gain[:, k * half_width : (k + 1) * half_width]
        return (total * own_gain).astype(BF16), jnp.sum(total * total, axis=1, keepdims=True)

    def place_rows(at):
        return pl.ds(at[1] * capacity, capacity)

    slot_rows = lax.broadcasted_iota(jnp.int32, (capacity, tokens), 0).astype(F32)

    def index(at):
        return 2 * at[0] + at[1]

    def pick(at, k):
        chosen = jnp.where(keys[pl.ds(peer(at), 1), :] == slot_rows, 1.0, 0.0).astype(BF16)
        return jnp.dot(chosen, scaled[k], preferred_element_type=F32).astype(BF16)

    def row_copy(at, k):
        p = index(at)
        return remote(
            picked.at[p, k],
            rows_ref.at[at[0], rank, k, place_rows(at)],
            row_send.at[p, k],
            row_recv.at[p, k],
            {"sp": peer(at)},
        )

    def spread(at, kind):
        owner, device = ((rank, across), (rank, partner), (across, partner))[kind]
        block = rows_ref.at[at[0], owner, :, place_rows(at)]
        p = index(at)
        return remote(
            block, block, spread_send.at[p, kind], spread_recv.at[p, kind], {"tp": device}
        )

    def spread_arrival(at, kind):
        owner = (across, partner, diagonal)[kind]
        block = rows_ref.at[at[0], owner, :, place_rows(at)]
        p = index(at)
        return remote(
            block, block, spread_send.at[p, kind], spread_recv.at[p, kind], {"tp": partner}
        )

    def fill_rows(at, k):
        if at == own:
            rows_ref[at[0], rank, k, place_rows(at)] = pick(at, k)
        else:
            picked[index(at), k] = pick(at, k)

    def send_rows(at, k):
        if at != own:
            row_copy(at, k).start()

    everyone = [(stage, place) for stage in range(stages) for place in range(2)]
    send_order = [(0, 1), own, (0, 0)] + [
        at for stage in range(1, stages) for at in ((stage, 1), (stage, 0)) if at != own
    ]
    first = send_order[:4]
    scaled, half_squares = [], []
    for k in range(2):
        block, square = scaled_half(k)
        scaled.append(block)
        half_squares.append(square)
        if k == 0:
            for at in first:
                fill_rows(at, k)
                send_rows(at, k)

    own_square = half_squares[0] + half_squares[1]
    squares[...] = jnp.transpose(jnp.broadcast_to(own_square, (tokens, LANES)))[0:8, :]
    square_copies = [
        remote(
            squares, squares_in.at[k], square_send.at[k], square_recv.at[k], {"tp": other}
        )
        for k, other in enumerate((partner, across, diagonal))
    ]
    for copy in square_copies:
        copy.start()
    for at in first:
        fill_rows(at, 1)
        send_rows(at, 1)
        if at == own:
            spread(at, 0).start()
            spread(at, 1).start()

    def scale_copy(at):
        p = index(at)
        return remote(
            scales.at[p], scales_in.at[p], scale_send.at[p], scale_recv.at[p], {"sp": peer(at)}
        )

    def send_scales():
        for copy in square_copies:
            copy.wait_recv()
        all_squares = squares[...] + squares_in[0] + squares_in[1] + squares_in[2]
        inv_rms = column_of(lax.rsqrt(all_squares / model_width + EPSILON)[0:1, :], LANES)
        inv_cols = jnp.concatenate([inv_rms] * (slot_lanes // LANES), axis=1)
        for at in send_order:
            row = jnp.sum(select[peer(at)].astype(F32) * inv_cols, axis=0, keepdims=True)
            if at == own:
                scales_in[index(at)] = jnp.broadcast_to(row, scales.shape[1:])
            else:
                scales[index(at)] = jnp.broadcast_to(row, scales.shape[1:])
                scale_copy(at).start()

    def direct(at):
        row_copy(at, 0).wait_recv()
        row_copy(at, 1).wait_recv()
        spread(at, 0).start()
        spread(at, 1).start()

    def relay(at):
        spread_arrival(at, 0).wait_recv()
        spread(at, 2).start()

    def half_copy(stage, k):
        return remote(
            down_share.at[stage, k],
            down_in.at[stage, k],
            half_send.at[stage, k],
            half_recv.at[stage, k],
            {"tp": partner},
        )

    arrived = set()

    def half_arrival(stage, k):
        if (stage, k) not in arrived:
            arrived.add((stage, k))
            half_copy(stage, k).wait_recv()

    def chip_rows(stage, which):
        pieces = [rows_ref[stage, 2 * which + k // 2, k % 2] for k in range(4)]
        return jnp.concatenate(pieces, axis=1)

    def expert_near(stage):
        for place in range(2):
            spread_arrival((stage, place), 1).wait_recv()
        block = chip_rows(stage, side)
        gate_part[stage % 2] = across_rows(gate_ref[:, chip_cols(side)], block)
        up_part[stage % 2] = across_rows(up_ref[:, chip_cols(side)], block)

    def expert_far(stage):
        for place in range(2):
            spread_arrival((stage, place), 2).wait_recv()
            if (stage, place) != own:
                scale_copy((stage, place)).wait_recv()
        block = chip_rows(stage, 1 - side)
        scale_lane = lax.broadcasted_iota(jnp.int32, scales.shape[1:], 1)
        scale = jnp.where(scale_lane < capacity, scales_in[2 * stage], scales_in[2 * stage + 1])
        scale = scale[0:1, 0 : 2 * capacity]
        gate_sum = gate_part[stage % 2] + across_rows(gate_ref[:, chip_cols(1 - side)], block)
        up_sum = up_part[stage % 2] + across_rows(up_ref[:, chip_cols(1 - side)], block)
        gate_sum = gate_sum * scale
        up_sum = up_sum * scale
        hidden = gate_sum / (1.0 + jnp.exp(-gate_sum)) * up_sum
        hidden_ref[stage % 2] = jnp.transpose(hidden).astype(BF16)

    def expert_down(stage, k):
        owner = (diagonal, partner, across, rank)[k]
        down_share[stage, k] = jnp.dot(
            hidden_ref[stage % 2], down_ref[:, cols(owner)], preferred_element_type=F32
        ).astype(BF16)
        if k < 2:
            half_copy(stage, k).start()

    def cross_copy(at):
        return remote(
            down_pair.at[at[0], place_rows(at)],
            down_pair_in.at[at[0], place_rows(at)],
            cross_send.at[index(at)],
            cross_recv.at[index(at)],
            {"tp": across},
        )

    def cross(at):
        stage, rows = at[0], place_rows(at)
        half_arrival(stage, 0)
        down_pair[stage, rows] = (
            down_share[stage, 2, rows].astype(F32) + down_in[stage, 0, rows].astype(F32)
        ).astype(BF16)
        cross_copy(at).start()

    def back_copy(at):
        p = index(at)
        return remote(
            finished.at[at[0], place_rows(at)],
            back.at[p],
            back_send.at[p],
            back_recv.at[p],
            {"sp": peer(at)},
        )

    def finish(at):
        stage, rows = at[0], place_rows(at)
        half_arrival(stage, 1)
        cross_copy(at).wait_recv()
        finished[stage, rows] = (
            down_share[stage, 3, rows].astype(F32)
            + down_in[stage, 1, rows].astype(F32)
            + down_pair_in[stage, rows].astype(F32)
        ).astype(BF16)
        if at != own:
            back_copy(at).start()

    def add_result(at):
        source = peer(at)
        if at == own:
            block = finished[at[0], place_rows(at)]
        else:
            back_copy(at).wait_recv()
            block = back[index(at)]
        weight = weight_cols[source][:, 0:1]
        stream[...] += weight * jnp.dot(
            select[source][:, 0:capacity], block, preferred_element_type=F32
        )

    send_scales()
    def send_later(at):
        for k in range(2):
            fill_rows(at, k)
            send_rows(at, k)

    def weights_here():
        for copy in local[1:]:
            copy.wait()

    def sends_done():
        for copy in halo_copies + to_partner + pair_copies + edge_copies + square_copies:
            copy.wait_send()
        for at in everyone:
            if at != own:
                row_copy(at, 0).wait_send()
                row_copy(at, 1).wait_send()
                scale_copy(at).wait_send()
            for kind in range(3):
                spread(at, kind).wait_send()
            cross_copy(at).wait_send()
        for stage in range(stages):
            half_copy(stage, 0).wait_send()
            half_copy(stage, 1).wait_send()

    on_blocks = {"S": send_later, "D": direct, "L": relay, "X": cross, "F": finish, "A": add_result}
    on_stages = {
        "N": expert_near,
        "G": expert_far,
        "Q": lambda stage: [expert_down(stage, k) for k in (0, 1)],
        "R": lambda stage: [expert_down(stage, k) for k in (2, 3)],
    }
    for step in plan_order(stages):
        if step == "W":
            weights_here()
        elif step == "E":
            sends_done()
        elif step[0] in on_stages:
            on_stages[step[0]](int(step[1]))
        else:
            on_blocks[step[0]]((int(step[1]), int(step[2])))
    out_ref[...] = stream[...].astype(BF16)

    for at in everyone:
        if at != own:
            back_copy(at).wait_send()


def fused(
    sp_count,
    in_gate,
    out_gate,
    values,
    conv_taps,
    doc_ids,
    residual,
    out_weight,
    norm_gain,
    routes,
    route_weights,
    expert_gate,
    expert_up,
    expert_down,
):
    channels, tokens = in_gate.shape
    model_width = residual.shape[1]
    width = model_width // 4
    capacity = 3 * tokens * routes.shape[1] // (2 * sp_count)
    slot_lanes = -(-2 * capacity // LANES) * LANES
    hidden = expert_gate.shape[2]
    stages = len(plan_stages(sp_count // 2))
    pair_rows = 2 * capacity
    vmem = pl.BlockSpec(memory_space=pltpu.VMEM)
    hbm = pl.BlockSpec(memory_space=pl.ANY)
    dma = pltpu.SemaphoreType.DMA
    return pl.pallas_call(
        functools.partial(layer_kernel, sp_count, capacity),
        out_shape=jax.ShapeDtypeStruct((tokens, width), BF16),
        in_specs=[vmem] * 5 + [hbm] + [vmem] * 4 + [hbm] * 3,
        out_specs=vmem,
        scratch_shapes=[
            pltpu.VMEM((hidden, model_width), BF16),
            pltpu.VMEM((hidden, model_width), BF16),
            pltpu.VMEM((hidden, model_width), BF16),
            pltpu.VMEM((model_width // LANES, LANES), F32),
            pltpu.VMEM((tokens, width), BF16),
            pltpu.VMEM((channels, tokens), BF16),
            pltpu.VMEM((16, channels), BF16),
            pltpu.VMEM((16, channels), BF16),
            pltpu.VMEM((1, tokens), jnp.int32),
            pltpu.VMEM((2, tokens, width), BF16),
            pltpu.VMEM((2, tokens, width), BF16),
            pltpu.VMEM((2, tokens, width // 2), BF16),
            pltpu.VMEM((2, tokens, width // 2), BF16),
            pltpu.VMEM((2, 16, width), BF16),
            pltpu.VMEM((2, 16, width), BF16),
            pltpu.VMEM((8, tokens), F32),
            pltpu.VMEM((3, 8, tokens), F32),
            pltpu.VMEM((sp_count, tokens), F32),
            pltpu.VMEM((sp_count, tokens, slot_lanes), BF16),
            pltpu.VMEM((sp_count, tokens, LANES), F32),
            pltpu.VMEM((sp_count, 8, slot_lanes), F32),
            pltpu.VMEM((sp_count, 8, slot_lanes), F32),
            pltpu.VMEM((tokens, width), F32),
            pltpu.VMEM((sp_count, 2, capacity, width // 2), BF16),
            pltpu.VMEM((stages, 4, 2, pair_rows, width // 2), BF16),
            pltpu.VMEM((2, hidden, pair_rows), F32),
            pltpu.VMEM((2, hidden, pair_rows), F32),
            pltpu.VMEM((2, pair_rows, hidden), BF16),
            pltpu.VMEM((stages, 4, pair_rows, width), BF16),
            pltpu.VMEM((stages, 2, pair_rows, width), BF16),
            pltpu.VMEM((stages, pair_rows, width), BF16),
            pltpu.VMEM((stages, pair_rows, width), BF16),
            pltpu.VMEM((stages, pair_rows, width), BF16),
            pltpu.VMEM((sp_count, capacity, width), BF16),
            dma((2,)),
            dma((2,)),
            dma((4,)),
            dma((3,)),
            dma((3,)),
            dma((4,)),
            dma((4,)),
            dma((2,)),
            dma((2,)),
            dma((3,)),
            dma((3,)),
            dma((sp_count,)),
            dma((sp_count,)),
            dma((sp_count, 2)),
            dma((sp_count, 2)),
            dma((sp_count, 3)),
            dma((sp_count, 3)),
            dma((stages, 2)),
            dma((stages, 2)),
            dma((sp_count,)),
            dma((sp_count,)),
            dma((sp_count,)),
            dma((sp_count,)),
        ],
        compiler_params=pltpu.CompilerParams(
            collective_id=0, has_side_effects=True, vmem_limit_bytes=60 * 1024 * 1024
        ),
    )(
        in_gate,
        out_gate,
        values,
        conv_taps,
        doc_ids.reshape(1, tokens),
        residual,
        out_weight,
        norm_gain.reshape(model_width // LANES, LANES),
        routes.T,
        route_weights.T,
        expert_gate.transpose(0, 2, 1),
        expert_up.transpose(0, 2, 1),
        expert_down,
    )


def solution(mesh):
    placed = (
        P("tp", "sp"),
        P("tp", "sp"),
        P("tp", "sp"),
        P(None, "tp"),
        P("sp"),
        P("sp", None),
        P("tp", None),
        P(),
        P("sp", None),
        P("sp", None),
        P("sp", None, "tp"),
        P("sp", None, "tp"),
        P("sp", "tp", None),
    )
    sp_count, tp_count = mesh.shape["sp"], mesh.shape["tp"]
    planes = sp_count // 2
    paired = tp_count == 4 and sp_count % 4 == 0 and planes & (planes - 1) == 0
    body = functools.partial(fused, sp_count) if paired else shards
    return jax.shard_map(
        body, mesh=mesh, in_specs=placed, out_specs=P("sp", "tp"), check_vma=False
    )
```
